256 devices in a mesh: ep: 128 (over z, y, x), tp: 2 (over core).
Axes of the slice: x: 4, y: 4, z: 8, core: 2. Of those that a mesh axis runs over, the one named last changes fastest.
Arguments:
- tokens: bfloat16 [2048, 2048], P('ep'), may hold values from -6 to 6
- lengths: int32 [2048], P('ep'), may hold values from 1024 to 8191
- prior_state: float32 [2048, 16, 64, 64], P('ep', 'tp'), may hold values from -2 to 2
- mix_gain: float32 [2048], replicated, may hold values from 0.1 to 1.9
- post_gain: float32 [2048], replicated, may hold values from 0.1 to 1.9
- ffn_gain: float32 [2048], replicated, may hold values from 0.1 to 1.9
- out_gain: float32 [2048], replicated, may hold values from 0.1 to 1.9
- query_weight: bfloat16 [2048, 1024], P('ep', 'tp'), may hold values from -0.125 to 0.125
- key_weight: bfloat16 [2048, 1024], P('ep', 'tp'), may hold values from -0.125 to 0.125
- value_weight: bfloat16 [2048, 1024], P('ep', 'tp'), may hold values from -0.125 to 0.125
- gate_weight: bfloat16 [2048, 1024], P('ep', 'tp'), may hold values from -0.125 to 0.125
- out_weight: bfloat16 [1024, 2048], P('tp', 'ep'), may hold values from -0.1875 to 0.1875
- routes: int32 [2048, 6], P('ep'), may hold values from 0 to 127, all different within a row; in each aligned block of 16 rows (0 to 15, 16 to 31, ...) at most 2 rows name the same one
- route_gates: float32 [2048, 6], P('ep'), may hold values from 0.1 to 0.9
- expert_gate: bfloat16 [128, 2048, 512], P('ep', None, 'tp'), may hold values from -0.125 to 0.125
- expert_up: bfloat16 [128, 2048, 512], P('ep', None, 'tp'), may hold values from -0.125 to 0.125
- expert_down: bfloat16 [128, 512, 2048], P('ep', 'tp'), may hold values from -0.25 to 0.25
- shared_gate: bfloat16 [2048, 512], P(None, 'tp'), may hold values from -0.125 to 0.125
- shared_up: bfloat16 [2048, 512], P(None, 'tp'), may hold values from -0.125 to 0.125
- shared_down: bfloat16 [512, 2048], P('tp'), may hold values from -0.25 to 0.25
Outputs:
- result: bfloat16 [2048, 2048], P('ep')
- new_state: float32 [2048, 16, 64, 64], P('ep', 'tp')
The draws below stay inside these ranges and needn't reach their ends.
Inputs may be any that keep to these rules, and one draw needn't show every extreme that they name: `routes`: each row names 6 different experts. In the rows of one device (aligned blocks of 16 rows) no expert is named more than 2 times, and in every draw some expert is named exactly 2 times in some block.
All inputs are finite; a program needn't handle non-finite values.
Results may differ from the reference program's by a relative error of at most 0.02.
Values may be sent and summed in bfloat16 or wider, within the bound.
No kernel may reach another device: no remote copies, remote signals or barrier semaphores. Data moves between devices by JAX's collectives and lax.ppermute only.
A program may use at most 128 MiB of HBM per device.

```python
import math
import jax
import jax.numpy as jnp
import numpy as np
from jax import lax

D = 2048
HEAD = 64
HEADS = 16
RW = 1024
FE = 512
FS = 512
TOPK = 6
SEQ_DEV = 16
TOKENS = 2048
EXPERTS = 128
CAP = 2
N_EP = 128
N_TP = 2


def with_ends(values, rng, least, top_value):
    place = [jax.random.randint(jax.random.fold_in(rng, axis), (), 0, length) for axis, length in enumerate(values.shape)]
    longest = values.shape.index(max(values.shape))
    beside = place[:longest] + [(place[longest] + 1) % values.shape[longest]] + place[longest + 1:]
    return values.at[tuple(place)].set(least).at[tuple(beside)].set(top_value)


def block_levels(key, extent, pieces, least, top_value):
    loudness = 1.0
    for position, shards_of in pieces:
        draws = jax.random.uniform(jax.random.fold_in(jax.random.fold_in(key, 6), position), (shards_of,), jnp.float32, least / len(pieces), top_value / len(pieces))
        loudness = loudness * jnp.repeat(jnp.exp(draws), extent[position] // shards_of).reshape((-1,) + (1,) * (len(extent) - 1 - position))
    return loudness


def assign_block(rng, own, number, rows, amount, top, reach, lean):
    sequence = jax.random.permutation(rng, amount)
    crowded, common = portions_of(amount, rows * top, reach, lean, True), portions_of(amount, rows * top, reach, lean, False)
    places = jnp.arange(amount)

    def named(sizes, offset_by):
        used = int((sizes > 0).sum())
        fixed = max(1, used // 4)
        passed = fixed + (places - fixed + offset_by * (used - fixed)) % max(1, amount - fixed)
        return jnp.zeros((amount,), jnp.int32).at[sequence[jnp.where(places < fixed, places, passed)]].set(jnp.asarray(sizes, jnp.int32))

    sizes = jnp.where(number % 4 == 0, named(crowded, number // 4), named(common, number - number // 4 - 1))
    mixed = jax.random.permutation(jax.random.fold_in(own, 3), amount)
    source_of, receiver = mixed[0:amount // 2 * 2:2], mixed[1:amount // 2 * 2:2]
    room = jnp.minimum(sizes[source_of] - 1, reach - sizes[receiver]) // 2
    room = jnp.where((source_of == sequence[0]) | (receiver == sequence[0]) | (sizes[receiver] == 0), 0, jnp.maximum(room, 0))
    passed = jax.random.randint(jax.random.fold_in(own, 4), (amount // 2,), 0, 1 << 20) % (room + 1)
    sizes = sizes.at[source_of].add(-passed).at[receiver].add(passed)
    members = jnp.searchsorted(jnp.cumsum(sizes), jnp.arange(rows * top), side="right").astype(jnp.int32)
    table = members.reshape(top, rows).T
    table = table[jax.random.permutation(jax.random.fold_in(own, 1), rows)]
    offset_by = jax.random.randint(jax.random.fold_in(own, 2), (rows, 1), 0, top)
    return jnp.take_along_axis(table, (jnp.arange(top)[None, :] + offset_by) % top, axis=1)


def portions_of(number_of, total, most, lean, full):
    weights = [(1 << 20) // math.isqrt(rank ** lean) + 1 for rank in range(1, number_of + 1)]
    largest = most if full else min(most, max(-(-total // number_of), total * weights[0] // sum(weights)))
    least = 1 if total - largest >= number_of - 1 else 0
    counts, rest = [largest] + [least] * (number_of - 1), total - largest - least * (number_of - 1)
    while rest > 0:
        movable = [i for i in range(1, number_of) if counts[i] < largest] or [i for i in range(1, number_of) if counts[i] < most]
        pool, budget = sum([weights[i] for i in movable]), rest
        for i in movable:
            extra = min(most - counts[i], max(1, budget * weights[i] // pool), rest)
            counts[i] = counts[i] + extra
            rest = rest - extra
    return np.array(counts)


def bell_draw(key, dims, spread, most, cuts=(), kind=jnp.bfloat16):
    array = spread * jax.random.normal(key, dims, jnp.float32)
    if cuts:
        array = array * block_levels(key, dims, cuts, -0.22, 0.18)
    return jnp.clip(array, -most, most).astype(kind)


def setup_inputs(seed: int = 0) -> dict:
    keys = jax.random.split(jax.random.key(seed), 21)
    tokens = bell_draw(keys[0], (TOKENS, D), 1.0, 6.0, ((0, 128),))
    lengths = with_ends(jax.random.randint(keys[1], (TOKENS,), 1024, 8192), jax.random.fold_in(keys[1], 1), 1024, 8191).astype(jnp.int32)
    prior_state = bell_draw(keys[2], (TOKENS, HEADS, HEAD, HEAD), 0.15, 2.0, ((0, 128), (1, 2)), jnp.float32)
    mix_gain = jnp.clip(1.0 + 0.18 * jax.random.normal(keys[3], (D,), jnp.float32), 0.1, 1.9)
    post_gain = jnp.clip(1.0 + 0.18 * jax.random.normal(keys[4], (D,), jnp.float32), 0.1, 1.9)
    ffn_gain = jnp.clip(1.0 + 0.18 * jax.random.normal(keys[5], (D,), jnp.float32), 0.1, 1.9)
    out_gain = jnp.clip(1.0 + 0.18 * jax.random.normal(keys[6], (D,), jnp.float32), 0.1, 1.9)
    query_weight = bell_draw(keys[7], (D, RW), D ** -0.5, 0.125, ((0, 128), (1, 2)))
    key_weight = bell_draw(keys[8], (D, RW), D ** -0.5, 0.125, ((0, 128), (1, 2)))
    value_weight = bell_draw(keys[9], (D, RW), D ** -0.5, 0.125, ((0, 128), (1, 2)))
    gate_weight = bell_draw(keys[10], (D, RW), D ** -0.5, 0.125, ((0, 128), (1, 2)))
    out_weight = bell_draw(keys[11], (RW, D), RW ** -0.5, 0.1875, ((0, 2), (1, 128)))
    routes_keys = jax.random.split(jax.random.fold_in(keys[12], 1), TOKENS // SEQ_DEV)
    routes_turns = jax.random.permutation(jax.random.fold_in(keys[12], 3), TOKENS // SEQ_DEV)
    routes = jax.vmap(lambda own, number: assign_block(jax.random.fold_in(keys[12], 2), own, number, SEQ_DEV, EXPERTS, TOPK, CAP, 2))(routes_keys, routes_turns).reshape((TOKENS, TOPK))
    route_gates = jnp.clip(0.1 + 0.79999997 * jax.random.uniform(keys[13], (TOKENS, TOPK), jnp.float32) ** block_levels(keys[13], (TOKENS, TOPK), ((0, 128),), -0.2, 0.2), 0.1, 0.9)
    expert_gate = bell_draw(keys[14], (EXPERTS, D, FE), D ** -0.5, 0.125, ((0, 128), (2, 2)))
    expert_up = bell_draw(keys[15], (EXPERTS, D, FE), D ** -0.5, 0.125, ((0, 128), (2, 2)))
    expert_down = bell_draw(keys[16], (EXPERTS, FE, D), FE ** -0.5, 0.25, ((0, 128), (1, 2)))
    shared_gate = bell_draw(keys[17], (D, FS), D ** -0.5, 0.125, ((1, 2),))
    shared_up = bell_draw(keys[18], (D, FS), D ** -0.5, 0.125, ((1, 2),))
    shared_down = bell_draw(keys[19], (FS, D), FS ** -0.5, 0.25, ((0, 2),))
    return {"tokens": tokens, "lengths": lengths, "prior_state": prior_state, "mix_gain": mix_gain, "post_gain": post_gain, "ffn_gain": ffn_gain, "out_gain": out_gain, "query_weight": query_weight, "key_weight": key_weight, "value_weight": value_weight, "gate_weight": gate_weight, "out_weight": out_weight, "routes": routes, "route_gates": route_gates, "expert_gate": expert_gate, "expert_up": expert_up, "expert_down": expert_down, "shared_gate": shared_gate, "shared_up": shared_up, "shared_down": shared_down}


EPS = 1e-06
THETA = 10000.0

def rounded(values):
    return lax.optimization_barrier(values.astype(jnp.bfloat16)).astype(jnp.float32)

def scaled_rows(values, gain_row):
    widened = values.astype(jnp.float32)
    return widened * lax.rsqrt(lax.optimization_barrier(jnp.mean(widened * widened, axis=-1, keepdims=True)) + EPS) * gain_row.astype(jnp.float32)

def rotate(vectors, lengths):
    half_dim = vectors.shape[-1] // 2
    frequency = THETA ** (-jnp.arange(half_dim, dtype=jnp.float32) / half_dim)
    angles = lengths.astype(jnp.float32)[:, None] * frequency[None, :]
    cosine = jnp.cos(angles)[:, None, :]
    sine_part = jnp.sin(angles)[:, None, :]
    leading = vectors[..., :half_dim]
    trailing = vectors[..., half_dim:]
    return jnp.concatenate([leading * cosine - trailing * sine_part, trailing * cosine + leading * sine_part], axis=-1)

def decay_table(head_count):
    head_order = jnp.arange(head_count, dtype=jnp.float32)
    return 1.0 - jnp.exp2(-5.0 - 7.0 * head_order / (head_count - 1))

def retain(queries, keys_new, values, out_gate, prior_state, lengths, decays):
    seq_count = queries.shape[0]
    head_count = decays.shape[0]
    layout = (seq_count, head_count, HEAD)
    rot_query = rotate(queries.astype(jnp.float32).reshape(layout), lengths)
    rot_key = rotate(keys_new.astype(jnp.float32).reshape(layout), lengths) * HEAD ** (-0.5)
    wide_values = values.astype(jnp.float32).reshape(layout)
    from_state = jnp.einsum('shd,shde->she', rot_query, prior_state, precision=lax.Precision.HIGHEST)
    self_term = lax.optimization_barrier(jnp.sum(rot_query * rot_key, axis=-1, keepdims=True))
    read_out = decays[None, :, None] * from_state + self_term * wide_values
    new_state = decays[None, :, None, None] * prior_state + rot_key[..., :, None] * wide_values[..., None, :]
    normed = read_out * lax.rsqrt(lax.optimization_barrier(jnp.mean(read_out * read_out, axis=-1, keepdims=True)) + EPS)
    gated_rows = normed.reshape(seq_count, head_count * HEAD) * jax.nn.silu(out_gate.astype(jnp.float32))
    return (gated_rows.astype(jnp.bfloat16), new_state)

def swiglu_split(inputs, w_gate, w_up, w_down):
    part_width = w_gate.shape[1] // N_TP
    running = jnp.zeros((inputs.shape[0], w_down.shape[1]), jnp.float32)
    for portion in range(N_TP):
        lower_row = portion * part_width
        gate_cols = jnp.dot(inputs, w_gate[:, lower_row:lower_row + part_width], preferred_element_type=jnp.float32)
        up_cols = jnp.dot(inputs, w_up[:, lower_row:lower_row + part_width], preferred_element_type=jnp.float32)
        hidden = (jax.nn.silu(gate_cols) * up_cols).astype(jnp.bfloat16)
        running = running + rounded(jnp.dot(hidden, w_down[lower_row:lower_row + part_width, :], preferred_element_type=jnp.float32))
    return running.astype(jnp.bfloat16)

def reference(tokens, lengths, prior_state, mix_gain, post_gain, ffn_gain, out_gain, query_weight, key_weight, value_weight, gate_weight, out_weight, routes, route_gates, expert_gate, expert_up, expert_down, shared_gate, shared_up, shared_down):
    normed = scaled_rows(tokens, mix_gain).astype(jnp.bfloat16)

    def project(weight_matrix):
        return jnp.dot(normed, weight_matrix, preferred_element_type=jnp.float32).astype(jnp.bfloat16)
    retained, new_state = retain(project(query_weight), project(key_weight), project(value_weight), project(gate_weight), prior_state, lengths, decay_table(HEADS))
    half_rows = RW // N_TP
    mixed_sum = jnp.zeros((TOKENS, D), jnp.float32)
    for portion in range(N_TP):
        lower_row = portion * half_rows
        mixed_sum = mixed_sum + rounded(jnp.dot(retained[:, lower_row:lower_row + half_rows], out_weight[lower_row:lower_row + half_rows, :], preferred_element_type=jnp.float32))
    middle = rounded(tokens.astype(jnp.float32) + scaled_rows(rounded(mixed_sum), post_gain))
    moe_in = scaled_rows(middle, ffn_gain).astype(jnp.bfloat16)
    padded_in = jnp.concatenate([moe_in, jnp.zeros((1, D), jnp.bfloat16)], axis=0)
    slot_total = N_EP * CAP

    def add_expert(running, expert_id):
        matched = routes == expert_id
        chosen = jnp.any(matched, axis=1)
        weights = lax.optimization_barrier(jnp.sum(jnp.where(matched, route_gates, jnp.zeros_like(route_gates)), axis=1))
        padded_w = jnp.concatenate([weights, jnp.zeros((1,), jnp.float32)])
        picked = jnp.nonzero(chosen, size=slot_total, fill_value=TOKENS)[0].astype(jnp.int32)
        outputs = swiglu_split(padded_in[picked], expert_gate[expert_id], expert_up[expert_id], expert_down[expert_id])
        return (running.at[picked].add(padded_w[picked][:, None] * outputs.astype(jnp.float32)), None)
    routed_all = lax.scan(add_expert, jnp.zeros((TOKENS + 1, D), jnp.float32), jnp.arange(EXPERTS, dtype=jnp.int32))[0]
    shared_out = swiglu_split(moe_in, shared_gate, shared_up, shared_down)
    mixture = shared_out.astype(jnp.float32) + routed_all[:TOKENS]
    result = (middle + scaled_rows(mixture, out_gain)).astype(jnp.bfloat16)
    return (result, new_state)
```

```python
import jax
import jax.numpy as jnp
from jax import lax
from jax.sharding import Mesh
from jax.sharding import PartitionSpec as P

HEAD = 64
HEADS = 16
Z, Y, X = "ep_0", "ep_1", "ep_2"
EP = (Z, Y, X)


EPS = 1e-06
THETA = 10000.0


def exchanged(blocks, axes):
    return lax.all_to_all(blocks, axes, split_axis=0, concat_axis=0, tiled=True)


def copies(value, count):
    return jnp.broadcast_to(value, (count, *value.shape))


def from_partner(value):
    return lax.ppermute(value, "tp", [(0, 1), (1, 0)])


def gathered_ahead(value, axis):
    size = lax.axis_size(axis)
    others = [
        lax.ppermute(value, axis, [((i + j) % size, i) for i in range(size)])
        for j in range(1, size)
    ]
    return jnp.stack([value, *others])


def rolled_lanes(rows, start):
    doubled = jnp.concatenate([rows, rows], axis=1)
    return lax.dynamic_slice_in_dim(doubled, start, rows.shape[1], 1)


def rounded(values):
    return lax.optimization_barrier(values.astype(jnp.bfloat16)).astype(jnp.float32)


def scaled_rows(values, gain_row):
    widened = values.astype(jnp.float32)
    return widened * lax.rsqrt(jnp.mean(widened * widened, axis=-1, keepdims=True) + EPS) * gain_row


def rotate(vectors, lengths):
    half_dim = vectors.shape[-1] // 2
    frequency = THETA ** (-jnp.arange(half_dim, dtype=jnp.float32) / half_dim)
    angles = lengths.astype(jnp.float32)[:, None] * frequency[None, :]
    cosine = jnp.cos(angles)[:, None, :]
    sine_part = jnp.sin(angles)[:, None, :]
    leading = vectors[..., :half_dim]
    trailing = vectors[..., half_dim:]
    return jnp.concatenate(
        [leading * cosine - trailing * sine_part, trailing * cosine + leading * sine_part], axis=-1
    )


def decay_table(head_count):
    head_order = jnp.arange(head_count, dtype=jnp.float32)
    return 1.0 - jnp.exp2(-5.0 - 7.0 * head_order / (head_count - 1))


def retain(queries, keys_new, values, out_gate, prior_state, lengths, decays):
    seq_count = queries.shape[0]
    head_count = decays.shape[0]
    layout = (seq_count, head_count, HEAD)
    rot_query = rotate(queries.astype(jnp.float32).reshape(layout), lengths)
    rot_key = rotate(keys_new.astype(jnp.float32).reshape(layout), lengths) * HEAD ** (-0.5)
    wide_values = values.astype(jnp.float32).reshape(layout)
    from_state = jnp.einsum("shd,shde->she", rot_query, prior_state)
    self_term = jnp.sum(rot_query * rot_key, axis=-1, keepdims=True)
    read_out = decays[None, :, None] * from_state + self_term * wide_values
    new_state = (
        decays[None, :, None, None] * prior_state
        + rot_key[..., :, None] * wide_values[..., None, :]
    )
    normed = read_out * lax.rsqrt(jnp.mean(read_out * read_out, axis=-1, keepdims=True) + EPS)
    gated_rows = normed.reshape(seq_count, head_count * HEAD) * jax.nn.silu(
        out_gate.astype(jnp.float32)
    )
    return (gated_rows.astype(jnp.bfloat16), new_state)


def on_device(
    tokens,
    lengths,
    prior_state,
    mix_gain,
    post_gain,
    ffn_gain,
    out_gain,
    query_weight,
    key_weight,
    value_weight,
    gate_weight,
    out_weight,
    routes,
    route_gates,
    expert_gate,
    expert_up,
    expert_down,
    shared_gate,
    shared_up,
    shared_down,
):
    seq_here, width = tokens.shape
    cols = query_weight.shape[1]
    depth, rows_y, rows_x = (lax.axis_size(axis) for axis in EP)
    experts_all = depth * rows_y * rows_x
    plane = rows_y * rows_x
    mine_z = lax.axis_index(Z)
    core = lax.axis_index("tp")
    slab = width // depth
    half = width // 2

    kinds = jnp.stack([query_weight, key_weight, value_weight, gate_weight])
    my_kind = exchanged(kinds, X)
    wout_rows = out_weight.T
    shard = jnp.concatenate([my_kind.reshape(-1, cols), wout_rows], axis=0)
    ahead = gathered_ahead(shard, Z)
    kind_rows = my_kind.shape[0] * my_kind.shape[1]
    kind_weight = ahead[:, :kind_rows].reshape(-1, cols)
    wout_z = ahead[:, kind_rows:]

    normed = scaled_rows(tokens, mix_gain).astype(jnp.bfloat16)
    turned = rolled_lanes(normed, mine_z * slab)
    by_y = turned.reshape(seq_here, depth, rows_y, -1).transpose(2, 0, 1, 3)
    by_y = by_y.reshape(rows_y, 1, seq_here, width // rows_y)
    outgoing_rows = jnp.broadcast_to(by_y, (rows_y, rows_x, seq_here, width // rows_y))
    plane_rows = exchanged(outgoing_rows.reshape(plane, seq_here, -1), (Y, X))
    projected = jnp.dot(
        plane_rows.reshape(plane * seq_here, -1), kind_weight, preferred_element_type=jnp.float32
    ).astype(jnp.bfloat16)
    parts = exchanged(projected.reshape(plane, seq_here, cols), (Y, X))
    parts = parts.reshape(rows_y, rows_x, seq_here, cols).astype(jnp.float32)
    queries, keys_new, values, out_gate = jnp.sum(parts, axis=0).astype(jnp.bfloat16)

    heads_here = cols // HEAD
    decays = lax.dynamic_slice_in_dim(decay_table(HEADS), core * heads_here, heads_here, 0)
    retained, new_state = retain(queries, keys_new, values, out_gate, prior_state, lengths, decays)

    wout_zx = exchanged(copies(wout_z.reshape(-1, cols), rows_x), X)
    wout_zx = wout_zx.reshape(rows_x, depth, -1, cols).transpose(1, 0, 2, 3).reshape(-1, cols)
    retained_y = exchanged(copies(retained, rows_y), Y).reshape(rows_y * seq_here, cols)
    partial_mix = lax.dot_general(
        retained_y, wout_zx, (((1,), (1,)), ((), ())), preferred_element_type=jnp.float32
    ).astype(jnp.bfloat16)
    to_both = partial_mix.reshape(rows_y, 1, seq_here, -1)
    to_both = jnp.broadcast_to(to_both, (rows_y, 2, *to_both.shape[2:]))
    halves = exchanged(to_both.reshape(2 * rows_y, seq_here, -1), (Y, "tp"))
    halves = halves.reshape(rows_y, 2, seq_here, depth, -1).astype(jnp.float32)
    mixed = jnp.sum(halves, axis=1).astype(jnp.bfloat16)
    mixed = mixed.transpose(1, 2, 0, 3).reshape(seq_here, width)
    mixed_sum = rounded(rolled_lanes(mixed, (depth - mine_z) * slab))
    middle = rounded(tokens.astype(jnp.float32) + scaled_rows(mixed_sum, post_gain))
    moe_in = scaled_rows(middle, ffn_gain).astype(jnp.bfloat16)

    topk_here = routes.shape[1]
    capacity = seq_here * topk_here // experts_all + 2
    slot_count = experts_all * capacity
    flat_routes = routes.reshape(-1)
    onehot = (flat_routes[:, None] == jnp.arange(experts_all, dtype=jnp.int32)[None, :]).astype(
        jnp.int32
    )
    earlier = jnp.cumsum(onehot, axis=0) - onehot
    ranks = jnp.sum(earlier * onehot, axis=1)
    slot_ids = flat_routes * capacity + ranks
    placing = (jnp.arange(slot_count, dtype=jnp.int32)[:, None] == slot_ids[None, :]).reshape(
        slot_count, seq_here, topk_here
    )
    dispatch_rows = jnp.any(placing, axis=2).astype(jnp.bfloat16)
    combine = jnp.sum(
        jnp.where(placing, route_gates[None, :, :], jnp.zeros((), jnp.float32)), axis=2
    ).T

    moe_half = lax.dynamic_slice_in_dim(moe_in, core * half, half, 1)
    outgoing = jnp.dot(dispatch_rows, moe_half, preferred_element_type=jnp.float32).astype(
        jnp.bfloat16
    )
    arrived = exchanged(outgoing.reshape(experts_all, capacity, half), EP)
    own_in = arrived.reshape(slot_count, half)
    other_in = from_partner(own_in)
    own_at, other_at = core * half, (1 - core) * half

    def both_halves(weight):
        own = lax.dynamic_slice_in_dim(weight, own_at, half, 0)
        other = lax.dynamic_slice_in_dim(weight, other_at, half, 0)
        return jnp.dot(own_in, own, preferred_element_type=jnp.float32) + jnp.dot(
            other_in, other, preferred_element_type=jnp.float32
        )

    hidden = (jax.nn.silu(both_halves(expert_gate[0])) * both_halves(expert_up[0])).astype(
        jnp.bfloat16
    )

    def down_half(rows, weight, at):
        piece = lax.dynamic_slice_in_dim(weight, at, half, 1)
        return jnp.dot(rows, piece, preferred_element_type=jnp.float32).astype(jnp.bfloat16)

    def summed_half(rows, weight):
        sent = from_partner(down_half(rows, weight, other_at))
        kept = down_half(rows, weight, own_at)
        return (kept.astype(jnp.float32) + sent.astype(jnp.float32)).astype(jnp.bfloat16)

    expert_sum = summed_half(hidden, expert_down[0])
    returned = exchanged(expert_sum.reshape(experts_all, capacity, half), EP)
    back_rows = returned.reshape(slot_count, half).astype(jnp.float32)
    routed = jnp.dot(combine, back_rows)
    shared_hidden = (
        jax.nn.silu(jnp.dot(moe_in, shared_gate, preferred_element_type=jnp.float32))
        * jnp.dot(moe_in, shared_up, preferred_element_type=jnp.float32)
    ).astype(jnp.bfloat16)
    shared_out = summed_half(shared_hidden, shared_down)
    mixture = shared_out.astype(jnp.float32) + routed
    other_mixture = from_partner(mixture)
    whole = jnp.where(
        core == 0,
        jnp.concatenate([mixture, other_mixture], axis=1),
        jnp.concatenate([other_mixture, mixture], axis=1),
    )
    result = (middle + scaled_rows(whole, out_gain)).astype(jnp.bfloat16)
    return (result, new_state)


def solution(mesh):
    finer = Mesh(mesh.devices.reshape(-1, 4, 4, mesh.shape["tp"]), ("ep_0", "ep_1", "ep_2", "tp"))
    in_specs = (
        P(EP, None),
        P(EP),
        P(EP, "tp", None, None),
        P(),
        P(),
        P(),
        P(),
        P(EP, "tp"),
        P(EP, "tp"),
        P(EP, "tp"),
        P(EP, "tp"),
        P("tp", EP),
        P(EP, None),
        P(EP, None),
        P(EP, None, "tp"),
        P(EP, None, "tp"),
        P(EP, "tp", None),
        P(None, "tp"),
        P(None, "tp"),
        P("tp", None),
    )
    out_specs = (P(EP, None), P(EP, "tp", None, None))
    return jax.shard_map(
        on_device, mesh=finer, in_specs=in_specs, out_specs=out_specs, check_vma=False
    )
```

```python
import jax
import jax.numpy as jnp
from jax import lax
from jax.sharding import Mesh
from jax.sharding import PartitionSpec as P

HEAD = 64
HEADS = 16
Z, Y, X = "ep_0", "ep_1", "ep_2"
EP = (Z, Y, X)


EPS = 1e-06
THETA = 10000.0


def exchanged(blocks, axes):
    return lax.all_to_all(blocks, axes, split_axis=0, concat_axis=0, tiled=True)


def copies(value, count):
    return jnp.broadcast_to(value, (count, *value.shape))


def from_partner(value):
    return lax.ppermute(value, "tp", [(0, 1), (1, 0)])


def from_ahead(value, axis, step):
    size = lax.axis_size(axis)
    return lax.ppermute(value, axis, [((i + step) % size, i) for i in range(size)])


def in_place_order(blocks, axis, dim):
    size = blocks.shape[dim]
    doubled = jnp.concatenate([blocks, blocks], axis=dim)
    start = (size - lax.axis_index(axis)) % size
    return lax.dynamic_slice_in_dim(doubled, start, size, dim)


def plane_tokens(by_y):
    size_y, size_x = by_y.shape[0], lax.axis_size(X)
    mine = lax.axis_index(Y)
    column = [lax.dynamic_index_in_dim(by_y, mine, 0, keepdims=False)]
    for step in range(1, size_y):
        behind = (mine - step) % size_y
        block = lax.dynamic_index_in_dim(by_y, behind, 0, keepdims=False)
        column.append(from_ahead(block, Y, step))
    column = in_place_order(jnp.stack(column), Y, 0)
    plane = jnp.stack([column] + [from_ahead(column, X, step) for step in range(1, size_x)])
    return in_place_order(plane, X, 0).swapaxes(0, 1)


def rounded(values):
    return lax.optimization_barrier(values.astype(jnp.bfloat16)).astype(jnp.float32)


def scaled_rows(values, gain_row):
    widened = values.astype(jnp.float32)
    return widened * lax.rsqrt(jnp.mean(widened * widened, axis=-1, keepdims=True) + EPS) * gain_row


def rotate(vectors, lengths):
    half_dim = vectors.shape[-1] // 2
    frequency = THETA ** (-jnp.arange(half_dim, dtype=jnp.float32) / half_dim)
    angles = lengths.astype(jnp.float32)[:, None] * frequency[None, :]
    cosine = jnp.cos(angles)[:, None, :]
    sine_part = jnp.sin(angles)[:, None, :]
    leading = vectors[..., :half_dim]
    trailing = vectors[..., half_dim:]
    return jnp.concatenate(
        [leading * cosine - trailing * sine_part, trailing * cosine + leading * sine_part], axis=-1
    )


def decay_table(head_count):
    head_order = jnp.arange(head_count, dtype=jnp.float32)
    return 1.0 - jnp.exp2(-5.0 - 7.0 * head_order / (head_count - 1))


def retain(queries, keys_new, values, out_gate, prior_state, lengths, decays):
    seq_count = queries.shape[0]
    head_count = decays.shape[0]
    layout = (seq_count, head_count, HEAD)
    rot_query = rotate(queries.astype(jnp.float32).reshape(layout), lengths)
    rot_key = rotate(keys_new.astype(jnp.float32).reshape(layout), lengths) * HEAD ** (-0.5)
    wide_values = values.astype(jnp.float32).reshape(layout)
    from_state = jnp.einsum("shd,shde->she", rot_query, prior_state)
    self_term = jnp.sum(rot_query * rot_key, axis=-1, keepdims=True)
    read_out = decays[None, :, None] * from_state + self_term * wide_values
    new_state = (
        decays[None, :, None, None] * prior_state
        + rot_key[..., :, None] * wide_values[..., None, :]
    )
    normed = read_out * lax.rsqrt(jnp.mean(read_out * read_out, axis=-1, keepdims=True) + EPS)
    gated_rows = normed.reshape(seq_count, head_count * HEAD) * jax.nn.silu(
        out_gate.astype(jnp.float32)
    )
    return (gated_rows.astype(jnp.bfloat16), new_state)


def on_device(
    tokens,
    lengths,
    prior_state,
    mix_gain,
    post_gain,
    ffn_gain,
    out_gain,
    query_weight,
    key_weight,
    value_weight,
    gate_weight,
    out_weight,
    routes,
    route_gates,
    expert_gate,
    expert_up,
    expert_down,
    shared_gate,
    shared_up,
    shared_down,
):
    seq_here, width = tokens.shape
    cols = query_weight.shape[1]
    depth, rows_y, rows_x = (lax.axis_size(axis) for axis in EP)
    experts_all = depth * rows_y * rows_x
    plane = rows_y * rows_x
    core = lax.axis_index("tp")
    half = width // 2

    kinds = jnp.stack([query_weight, key_weight, value_weight, gate_weight])
    wout_rows = copies(out_weight.T, rows_x)
    sent = copies(jnp.concatenate([kinds, wout_rows], axis=1), depth)
    held = exchanged(sent.reshape(depth * rows_x, -1, cols), (Z, X))
    kind_rows = query_weight.shape[0]
    kind_weight = held[:, :kind_rows].reshape(-1, cols)
    wout_zx = held[:, kind_rows:].reshape(-1, cols)

    normed = scaled_rows(tokens, mix_gain).astype(jnp.bfloat16)
    by_y = normed.reshape(seq_here, depth, rows_y, -1).transpose(2, 0, 1, 3)
    plane_rows = plane_tokens(by_y.reshape(rows_y, seq_here, width // rows_y))
    projected = jnp.dot(
        plane_rows.reshape(plane * seq_here, -1), kind_weight, preferred_element_type=jnp.float32
    ).astype(jnp.bfloat16)
    parts = exchanged(projected.reshape(plane, seq_here, cols), (Y, X))
    parts = parts.reshape(rows_y, rows_x, seq_here, cols).astype(jnp.float32)
    queries, keys_new, values, out_gate = jnp.sum(parts, axis=0).astype(jnp.bfloat16)

    heads_here = cols // HEAD
    decays = lax.dynamic_slice_in_dim(decay_table(HEADS), core * heads_here, heads_here, 0)
    retained, new_state = retain(queries, keys_new, values, out_gate, prior_state, lengths, decays)

    retained_y = exchanged(copies(retained, rows_y), Y).reshape(rows_y * seq_here, cols)
    partial_mix = lax.dot_general(
        retained_y, wout_zx, (((1,), (1,)), ((), ())), preferred_element_type=jnp.float32
    ).astype(jnp.bfloat16)
    to_both = partial_mix.reshape(rows_y, 1, seq_here, -1)
    to_both = jnp.broadcast_to(to_both, (rows_y, 2, *to_both.shape[2:]))
    halves = exchanged(to_both.reshape(2 * rows_y, seq_here, -1), (Y, "tp"))
    halves = halves.reshape(rows_y, 2, seq_here, depth, -1).astype(jnp.float32)
    mixed = jnp.sum(halves, axis=1).astype(jnp.bfloat16)
    mixed = mixed.transpose(1, 2, 0, 3).reshape(seq_here, width)
    mixed_sum = rounded(mixed)
    middle = rounded(tokens.astype(jnp.float32) + scaled_rows(mixed_sum, post_gain))
    moe_in = scaled_rows(middle, ffn_gain).astype(jnp.bfloat16)

    topk_here = routes.shape[1]
    capacity = seq_here * topk_here // experts_all + 2
    slot_count = experts_all * capacity
    flat_routes = routes.reshape(-1)
    onehot = (flat_routes[:, None] == jnp.arange(experts_all, dtype=jnp.int32)[None, :]).astype(
        jnp.int32
    )
    earlier = jnp.cumsum(onehot, axis=0) - onehot
    ranks = jnp.sum(earlier * onehot, axis=1)
    slot_ids = flat_routes * capacity + ranks
    placing = (jnp.arange(slot_count, dtype=jnp.int32)[:, None] == slot_ids[None, :]).reshape(
        slot_count, seq_here, topk_here
    )
    dispatch_rows = jnp.any(placing, axis=2).astype(jnp.bfloat16)
    combine = jnp.sum(
        jnp.where(placing, route_gates[None, :, :], jnp.zeros((), jnp.float32)), axis=2
    ).T

    moe_half = lax.dynamic_slice_in_dim(moe_in, core * half, half, 1)
    outgoing = jnp.dot(dispatch_rows, moe_half, preferred_element_type=jnp.float32).astype(
        jnp.bfloat16
    )
    arrived = exchanged(outgoing.reshape(experts_all, capacity, half), EP)
    own_at, other_at = core * half, (1 - core) * half

    def down_halves(weight):
        return tuple(lax.dynamic_slice_in_dim(weight, at, half, 1) for at in (own_at, other_at))

    def up_halves():
        both = (expert_gate[0], expert_up[0])
        return tuple(
            jnp.concatenate([lax.dynamic_slice_in_dim(w, at, half, 0) for w in both], axis=1)
            for at in (own_at, other_at)
        )

    def summed_half(rows, halves):
        kept, sent = (
            jnp.dot(rows, piece, preferred_element_type=jnp.float32).astype(jnp.bfloat16)
            for piece in halves
        )
        got = from_partner(sent)
        return (kept.astype(jnp.float32) + got.astype(jnp.float32)).astype(jnp.bfloat16)

    shared_hidden = (
        jax.nn.silu(jnp.dot(moe_in, shared_gate, preferred_element_type=jnp.float32))
        * jnp.dot(moe_in, shared_up, preferred_element_type=jnp.float32)
    ).astype(jnp.bfloat16)
    shared_out = summed_half(shared_hidden, down_halves(shared_down))

    beside = (shared_out, new_state, up_halves(), down_halves(expert_down[0]))
    arrived, beside = lax.optimization_barrier((arrived, beside))
    shared_out, new_state, up_pieces, down_pieces = beside

    own_in = arrived.reshape(slot_count, half)
    other_in = from_partner(own_in)
    lifted = jnp.dot(own_in, up_pieces[0], preferred_element_type=jnp.float32) + jnp.dot(
        other_in, up_pieces[1], preferred_element_type=jnp.float32
    )
    gate_part, up_part = jnp.split(lifted, 2, axis=1)
    hidden = (jax.nn.silu(gate_part) * up_part).astype(jnp.bfloat16)
    expert_sum = summed_half(hidden, down_pieces)
    returned = exchanged(expert_sum.reshape(experts_all, capacity, half), EP)
    back_rows = returned.reshape(slot_count, half).astype(jnp.float32)
    routed = jnp.dot(combine, back_rows)
    mixture = shared_out.astype(jnp.float32) + routed
    other_mixture = from_partner(mixture)
    whole = jnp.where(
        core == 0,
        jnp.concatenate([mixture, other_mixture], axis=1),
        jnp.concatenate([other_mixture, mixture], axis=1),
    )
    result = (middle + scaled_rows(whole, out_gain)).astype(jnp.bfloat16)
    return (result, new_state)


def solution(mesh):
    finer = Mesh(mesh.devices.reshape(-1, 4, 4, mesh.shape["tp"]), ("ep_0", "ep_1", "ep_2", "tp"))
    in_specs = (
        P(EP, None),
        P(EP),
        P(EP, "tp", None, None),
        P(),
        P(),
        P(),
        P(),
        P(EP, "tp"),
        P(EP, "tp"),
        P(EP, "tp"),
        P(EP, "tp"),
        P("tp", EP),
        P(EP, None),
        P(EP, None),
        P(EP, None, "tp"),
        P(EP, None, "tp"),
        P(EP, "tp", None),
        P(None, "tp"),
        P(None, "tp"),
        P("tp", None),
    )
    out_specs = (P(EP, None), P(EP, "tp", None, None))

    return jax.shard_map(
        on_device, mesh=finer, in_specs=in_specs, out_specs=out_specs, check_vma=False
    )
```

```python
import jax
import jax.numpy as jnp
from jax import lax
from jax.sharding import Mesh
from jax.sharding import PartitionSpec as P

HEAD = 64
HEADS = 16
Z, Y, X = "ep_0", "ep_1", "ep_2"
EP = (Z, Y, X)


EPS = 1e-06
THETA = 10000.0


def exchanged(blocks, axes):
    return lax.all_to_all(blocks, axes, split_axis=0, concat_axis=0, tiled=True)


def copies(value, count):
    return jnp.broadcast_to(value, (count, *value.shape))


def from_partner(value):
    return lax.ppermute(value, "tp", [(0, 1), (1, 0)])


def rolled_lanes(rows, start):
    doubled = jnp.concatenate([rows, rows], axis=1)
    return lax.dynamic_slice_in_dim(doubled, start, rows.shape[1], 1)


def from_ahead(value, axis, step):
    size = lax.axis_size(axis)
    return lax.ppermute(value, axis, [((i + step) % size, i) for i in range(size)])


def in_place_order(blocks, axis, dim):
    size = blocks.shape[dim]
    doubled = jnp.concatenate([blocks, blocks], axis=dim)
    start = (size - lax.axis_index(axis)) % size
    return lax.dynamic_slice_in_dim(doubled, start, size, dim)


def plane_tokens(by_y):
    size_y, size_x = by_y.shape[0], lax.axis_size(X)
    mine = lax.axis_index(Y)
    column = [lax.dynamic_index_in_dim(by_y, mine, 0, keepdims=False)]
    for step in range(1, size_y):
        behind = (mine - step) % size_y
        block = lax.dynamic_index_in_dim(by_y, behind, 0, keepdims=False)
        column.append(from_ahead(block, Y, step))
    column = in_place_order(jnp.stack(column), Y, 0)
    plane = jnp.stack([column] + [from_ahead(column, X, step) for step in range(1, size_x)])
    return in_place_order(plane, X, 0).swapaxes(0, 1)


def rounded(values):
    return lax.optimization_barrier(values.astype(jnp.bfloat16)).astype(jnp.float32)


def scaled_rows(values, gain_row):
    widened = values.astype(jnp.float32)
    return widened * lax.rsqrt(jnp.mean(widened * widened, axis=-1, keepdims=True) + EPS) * gain_row


def rotate(vectors, lengths):
    half_dim = vectors.shape[-1] // 2
    frequency = THETA ** (-jnp.arange(half_dim, dtype=jnp.float32) / half_dim)
    angles = lengths.astype(jnp.float32)[:, None] * frequency[None, :]
    cosine = jnp.cos(angles)[:, None, :]
    sine_part = jnp.sin(angles)[:, None, :]
    leading = vectors[..., :half_dim]
    trailing = vectors[..., half_dim:]
    return jnp.concatenate(
        [leading * cosine - trailing * sine_part, trailing * cosine + leading * sine_part], axis=-1
    )


def decay_table(head_count):
    head_order = jnp.arange(head_count, dtype=jnp.float32)
    return 1.0 - jnp.exp2(-5.0 - 7.0 * head_order / (head_count - 1))


def retain(queries, keys_new, values, out_gate, prior_state, lengths, decays):
    seq_count = queries.shape[0]
    head_count = decays.shape[0]
    layout = (seq_count, head_count, HEAD)
    rot_query = rotate(queries.astype(jnp.float32).reshape(layout), lengths)
    rot_key = rotate(keys_new.astype(jnp.float32).reshape(layout), lengths) * HEAD ** (-0.5)
    wide_values = values.astype(jnp.float32).reshape(layout)
    from_state = jnp.einsum("shd,shde->she", rot_query, prior_state)
    self_term = jnp.sum(rot_query * rot_key, axis=-1, keepdims=True)
    read_out = decays[None, :, None] * from_state + self_term * wide_values
    normed = read_out * lax.rsqrt(jnp.mean(read_out * read_out, axis=-1, keepdims=True) + EPS)
    gated_rows = normed.reshape(seq_count, head_count * HEAD) * jax.nn.silu(
        out_gate.astype(jnp.float32)
    )
    return (gated_rows.astype(jnp.bfloat16), rot_key, wide_values)


def next_state(decays, prior_state, rot_key, wide_values):
    return (
        decays[None, :, None, None] * prior_state
        + rot_key[..., :, None] * wide_values[..., None, :]
    )


def on_device(
    tokens,
    lengths,
    prior_state,
    mix_gain,
    post_gain,
    ffn_gain,
    out_gain,
    query_weight,
    key_weight,
    value_weight,
    gate_weight,
    out_weight,
    routes,
    route_gates,
    expert_gate,
    expert_up,
    expert_down,
    shared_gate,
    shared_up,
    shared_down,
):
    seq_here, width = tokens.shape
    cols = query_weight.shape[1]
    depth, rows_y, rows_x = (lax.axis_size(axis) for axis in EP)
    experts_all = depth * rows_y * rows_x
    plane = rows_y * rows_x
    core = lax.axis_index("tp")

    kinds = jnp.stack([query_weight, key_weight, value_weight, gate_weight])
    share = cols // rows_x
    wout_parts = out_weight.reshape(rows_x, share, -1).swapaxes(1, 2)
    sent = copies(jnp.concatenate([kinds, wout_parts], axis=2), depth)
    held = exchanged(sent.reshape(depth * rows_x, -1, cols + share), (Z, X))
    held = held.reshape(-1, cols + share)
    kind_weight = held[:, :cols]
    wout_part = held[:, cols:]
    others = [from_ahead(wout_part, X, step) for step in range(1, rows_x)]
    wout_turned = jnp.concatenate([wout_part, *others], axis=1)

    normed = scaled_rows(tokens, mix_gain).astype(jnp.bfloat16)
    by_y = normed.reshape(seq_here, depth, rows_y, -1).transpose(2, 0, 1, 3)
    plane_rows = plane_tokens(by_y.reshape(rows_y, seq_here, width // rows_y))
    projected = jnp.dot(
        plane_rows.reshape(plane * seq_here, -1), kind_weight, preferred_element_type=jnp.float32
    ).astype(jnp.bfloat16)
    parts = exchanged(projected.reshape(plane, seq_here, cols), (Y, X))
    parts = parts.reshape(rows_y, rows_x, seq_here, cols).astype(jnp.float32)
    queries, keys_new, values, out_gate = jnp.sum(parts, axis=0).astype(jnp.bfloat16)

    heads_here = cols // HEAD
    decays = lax.dynamic_slice_in_dim(decay_table(HEADS), core * heads_here, heads_here, 0)
    retained, rot_key, wide_values = retain(
        queries, keys_new, values, out_gate, prior_state, lengths, decays
    )

    turned = rolled_lanes(retained, lax.axis_index(X) * share)
    retained_y = exchanged(copies(turned, rows_y), Y).reshape(rows_y * seq_here, cols)
    partial_mix = lax.dot_general(
        retained_y, wout_turned, (((1,), (1,)), ((), ())), preferred_element_type=jnp.float32
    ).astype(jnp.bfloat16)
    to_both = partial_mix.reshape(rows_y, 1, seq_here, -1)
    to_both = jnp.broadcast_to(to_both, (rows_y, 2, *to_both.shape[2:]))
    halves = exchanged(to_both.reshape(2 * rows_y, seq_here, -1), (Y, "tp"))
    halves = halves.reshape(rows_y, 2, seq_here, depth, -1).astype(jnp.float32)
    mixed = jnp.sum(halves, axis=1).astype(jnp.bfloat16)
    mixed = mixed.transpose(1, 2, 0, 3).reshape(seq_here, width)
    mixed_sum = rounded(mixed)
    middle = rounded(tokens.astype(jnp.float32) + scaled_rows(mixed_sum, post_gain))
    moe_in = scaled_rows(middle, ffn_gain).astype(jnp.bfloat16)

    flat_routes = routes.reshape(-1)
    onehot = (flat_routes[:, None] == jnp.arange(experts_all, dtype=jnp.int32)[None, :]).astype(
        jnp.int32
    )
    earlier = jnp.cumsum(onehot, axis=0) - onehot
    ranks = jnp.sum(earlier * onehot, axis=1)
    mine = jnp.where(ranks == core, flat_routes, -1)
    placing = (jnp.arange(experts_all, dtype=jnp.int32)[:, None] == mine[None, :]).reshape(
        experts_all, seq_here, -1
    )
    dispatch_rows = jnp.any(placing, axis=2).astype(jnp.bfloat16)
    combine = jnp.sum(
        jnp.where(placing, route_gates[None, :, :], jnp.zeros((), jnp.float32)), axis=2
    ).T

    outgoing = jnp.dot(dispatch_rows, moe_in, preferred_element_type=jnp.float32).astype(
        jnp.bfloat16
    )
    outgoing, moe_beside, state_beside = lax.optimization_barrier((outgoing, moe_in, prior_state))
    arrived = exchanged(outgoing.reshape(experts_all, 2, -1), EP)

    def lifted(rows, w_gate, w_up):
        return (
            jax.nn.silu(jnp.dot(rows, w_gate, preferred_element_type=jnp.float32))
            * jnp.dot(rows, w_up, preferred_element_type=jnp.float32)
        ).astype(jnp.bfloat16)

    def lowered(rows, w_down):
        return jnp.dot(rows, w_down, preferred_element_type=jnp.float32).astype(jnp.bfloat16)

    new_state = next_state(decays, state_beside, rot_key, wide_values)
    shared_part = lowered(lifted(moe_beside, shared_gate, shared_up), shared_down)
    arrived, shared_part, new_state = lax.optimization_barrier((arrived, shared_part, new_state))

    own_in = arrived.reshape(experts_all, width)
    other_in = from_partner(own_in)
    own_hidden = lifted(own_in, expert_gate[0], expert_up[0])
    own_hidden, other_in = lax.optimization_barrier((own_hidden, other_in))
    other_hidden = lifted(other_in, expert_gate[0], expert_up[0])
    got = from_partner(lowered(other_hidden, expert_down[0]))
    own_sum = lowered(own_hidden, expert_down[0]).astype(jnp.float32) + got.astype(jnp.float32)
    own_sum = own_sum.astype(jnp.bfloat16)
    returned = exchanged(own_sum.reshape(experts_all, 2, -1), EP)
    back_rows = returned.reshape(experts_all, width).astype(jnp.float32)
    mixture_part = jnp.dot(combine, back_rows) + shared_part.astype(jnp.float32)
    mixture = mixture_part + from_partner(mixture_part)
    result = (middle + scaled_rows(mixture, out_gain)).astype(jnp.bfloat16)
    return (result, new_state)


def solution(mesh):
    finer = Mesh(mesh.devices.reshape(-1, 4, 4, mesh.shape["tp"]), ("ep_0", "ep_1", "ep_2", "tp"))
    in_specs = (
        P(EP, None),
        P(EP),
        P(EP, "tp", None, None),
        P(),
        P(),
        P(),
        P(),
        P(EP, "tp"),
        P(EP, "tp"),
        P(EP, "tp"),
        P(EP, "tp"),
        P("tp", EP),
        P(EP, None),
        P(EP, None),
        P(EP, None, "tp"),
        P(EP, None, "tp"),
        P(EP, "tp", None),
        P(None, "tp"),
        P(None, "tp"),
        P("tp", None),
    )
    out_specs = (P(EP, None), P(EP, "tp", None, None))

    return jax.shard_map(
        on_device, mesh=finer, in_specs=in_specs, out_specs=out_specs, check_vma=False
    )
```

```python
import jax
import jax.numpy as jnp
from jax import lax
from jax.sharding import Mesh
from jax.sharding import PartitionSpec as P

HEAD = 64
HEADS = 16
Z, Y, X = "ep_0", "ep_1", "ep_2"
EP = (Z, Y, X)


EPS = 1e-06
THETA = 10000.0


def exchanged(blocks, axes):
    return lax.all_to_all(blocks, axes, split_axis=0, concat_axis=0, tiled=True)


def copies(value, count):
    return jnp.broadcast_to(value, (count, *value.shape))


def from_partner(value):
    return lax.ppermute(value, "tp", [(0, 1), (1, 0)])


def rolled_lanes(rows, start):
    doubled = jnp.concatenate([rows, rows], axis=1)
    return lax.dynamic_slice_in_dim(doubled, start, rows.shape[1], 1)


def from_ahead(value, axis, step):
    size = lax.axis_size(axis)
    return lax.ppermute(value, axis, [((i + step) % size, i) for i in range(size)])


def in_place_order(blocks, axis, dim):
    size = blocks.shape[dim]
    doubled = jnp.concatenate([blocks, blocks], axis=dim)
    start = (size - lax.axis_index(axis)) % size
    return lax.dynamic_slice_in_dim(doubled, start, size, dim)


def plane_tokens(by_y):
    size_y, size_x = by_y.shape[0], lax.axis_size(X)
    mine = lax.axis_index(Y)
    column = [lax.dynamic_index_in_dim(by_y, mine, 0, keepdims=False)]
    for step in range(1, size_y):
        behind = (mine - step) % size_y
        block = lax.dynamic_index_in_dim(by_y, behind, 0, keepdims=False)
        column.append(from_ahead(block, Y, step))
    column = in_place_order(jnp.stack(column), Y, 0)
    others = [from_ahead(column, X, step) for step in range(1, size_x)]
    plane = jnp.stack([column, *others])
    return in_place_order(plane, X, 0).swapaxes(0, 1)


def rounded(values):
    return lax.optimization_barrier(values.astype(jnp.bfloat16)).astype(jnp.float32)


def scaled_rows(values, gain_row):
    widened = values.astype(jnp.float32)
    return widened * lax.rsqrt(jnp.mean(widened * widened, axis=-1, keepdims=True) + EPS) * gain_row


def rotate(vectors, lengths):
    half_dim = vectors.shape[-1] // 2
    frequency = THETA ** (-jnp.arange(half_dim, dtype=jnp.float32) / half_dim)
    angles = lengths.astype(jnp.float32)[:, None] * frequency[None, :]
    cosine = jnp.cos(angles)[:, None, :]
    sine_part = jnp.sin(angles)[:, None, :]
    leading = vectors[..., :half_dim]
    trailing = vectors[..., half_dim:]
    return jnp.concatenate(
        [leading * cosine - trailing * sine_part, trailing * cosine + leading * sine_part], axis=-1
    )


def decay_table(head_count):
    head_order = jnp.arange(head_count, dtype=jnp.float32)
    return 1.0 - jnp.exp2(-5.0 - 7.0 * head_order / (head_count - 1))


def retain(queries, keys_new, values, out_gate, prior_state, lengths, decays):
    seq_count = queries.shape[0]
    head_count = decays.shape[0]
    layout = (seq_count, head_count, HEAD)
    rot_query = rotate(queries.astype(jnp.float32).reshape(layout), lengths)
    rot_key = rotate(keys_new.astype(jnp.float32).reshape(layout), lengths) * HEAD ** (-0.5)
    wide_values = values.astype(jnp.float32).reshape(layout)
    from_state = jnp.einsum("shd,shde->she", rot_query, prior_state)
    self_term = jnp.sum(rot_query * rot_key, axis=-1, keepdims=True)
    read_out = decays[None, :, None] * from_state + self_term * wide_values
    normed = read_out * lax.rsqrt(jnp.mean(read_out * read_out, axis=-1, keepdims=True) + EPS)
    gated_rows = normed.reshape(seq_count, head_count * HEAD) * jax.nn.silu(
        out_gate.astype(jnp.float32)
    )
    return (gated_rows.astype(jnp.bfloat16), rot_key, wide_values)


def next_state(decays, prior_state, rot_key, wide_values):
    return (
        decays[None, :, None, None] * prior_state
        + rot_key[..., :, None] * wide_values[..., None, :]
    )


def on_device(
    tokens,
    lengths,
    prior_state,
    mix_gain,
    post_gain,
    ffn_gain,
    out_gain,
    query_weight,
    key_weight,
    value_weight,
    gate_weight,
    out_weight,
    routes,
    route_gates,
    expert_gate,
    expert_up,
    expert_down,
    shared_gate,
    shared_up,
    shared_down,
):
    seq_here, width = tokens.shape
    cols = query_weight.shape[1]
    depth, rows_y, rows_x = (lax.axis_size(axis) for axis in EP)
    experts_all = depth * rows_y * rows_x
    plane = rows_y * rows_x
    core = lax.axis_index("tp")

    kinds = jnp.stack([query_weight, key_weight, value_weight, gate_weight])
    share = cols // rows_x
    wout_parts = out_weight.reshape(rows_x, share, -1).swapaxes(1, 2)
    sent = copies(jnp.concatenate([kinds, wout_parts], axis=2), depth)
    held = exchanged(sent.reshape(depth * rows_x, -1, cols + share), (Z, X))
    held = held.reshape(-1, cols + share)
    kind_weight = held[:, :cols]
    wout_part = held[:, cols:]
    others = [from_ahead(wout_part, X, step) for step in range(1, rows_x)]

    wide_tokens = tokens.astype(jnp.float32)
    gained = (wide_tokens * mix_gain).astype(jnp.bfloat16)
    by_y = gained.reshape(seq_here, depth, rows_y, -1).transpose(2, 0, 1, 3)
    plane_rows = plane_tokens(by_y.reshape(rows_y, seq_here, width // rows_y))
    projected = jnp.dot(
        plane_rows.reshape(plane * seq_here, -1), kind_weight, preferred_element_type=jnp.float32
    ).astype(jnp.bfloat16)
    projected, routes, route_gates = lax.optimization_barrier((projected, routes, route_gates))
    parts = exchanged(projected.reshape(plane, seq_here, cols), (Y, X))
    flat_routes = routes.reshape(-1)
    onehot = (flat_routes[:, None] == jnp.arange(experts_all, dtype=jnp.int32)[None, :]).astype(
        jnp.int32
    )
    earlier = jnp.cumsum(onehot, axis=0) - onehot
    ranks = jnp.sum(earlier * onehot, axis=1)
    mine = jnp.where(ranks == core, flat_routes, -1)
    placing = (jnp.arange(experts_all, dtype=jnp.int32)[:, None] == mine[None, :]).reshape(
        experts_all, seq_here, -1
    )
    dispatch_rows = jnp.any(placing, axis=2).astype(jnp.bfloat16)
    combine = jnp.sum(
        jnp.where(placing, route_gates[None, :, :], jnp.zeros((), jnp.float32)), axis=2
    ).T

    row_scale = lax.rsqrt(jnp.mean(wide_tokens * wide_tokens, axis=-1, keepdims=True) + EPS)

    parts, dispatch_rows, combine, row_scale = lax.optimization_barrier(
        (parts, dispatch_rows, combine, row_scale)
    )
    parts = parts.reshape(rows_y, rows_x, seq_here, cols).astype(jnp.float32)
    queries, keys_new, values, out_gate = (jnp.sum(parts, axis=0) * row_scale).astype(jnp.bfloat16)

    heads_here = cols // HEAD
    decays = lax.dynamic_slice_in_dim(decay_table(HEADS), core * heads_here, heads_here, 0)
    retained, rot_key, wide_values = retain(
        queries, keys_new, values, out_gate, prior_state, lengths, decays
    )

    turned = rolled_lanes(retained, lax.axis_index(X) * share)
    turned, others = lax.optimization_barrier((turned, others))
    wout_turned = jnp.concatenate([wout_part, *others], axis=1)
    retained_y = exchanged(copies(turned, rows_y), Y).reshape(rows_y * seq_here, cols)
    partial_mix = lax.dot_general(
        retained_y, wout_turned, (((1,), (1,)), ((), ())), preferred_element_type=jnp.float32
    ).astype(jnp.bfloat16)
    to_both = partial_mix.reshape(rows_y, 1, seq_here, -1)
    to_both = jnp.broadcast_to(to_both, (rows_y, 2, *to_both.shape[2:]))
    halves = exchanged(to_both.reshape(2 * rows_y, seq_here, -1), (Y, "tp"))
    halves = halves.reshape(rows_y, 2, seq_here, depth, -1).astype(jnp.float32)
    mixed = jnp.sum(halves, axis=1).astype(jnp.bfloat16)
    mixed = mixed.transpose(1, 2, 0, 3).reshape(seq_here, width)
    mixed_sum = rounded(mixed)
    middle = rounded(tokens.astype(jnp.float32) + scaled_rows(mixed_sum, post_gain))
    moe_in = scaled_rows(middle, ffn_gain).astype(jnp.bfloat16)

    outgoing = jnp.dot(dispatch_rows, moe_in, preferred_element_type=jnp.float32).astype(
        jnp.bfloat16
    )
    outgoing, moe_beside, state_beside = lax.optimization_barrier((outgoing, moe_in, prior_state))
    arrived = exchanged(outgoing.reshape(experts_all, 2, -1), EP)

    def lifted(rows, w_gate, w_up):
        return (
            jax.nn.silu(jnp.dot(rows, w_gate, preferred_element_type=jnp.float32))
            * jnp.dot(rows, w_up, preferred_element_type=jnp.float32)
        ).astype(jnp.bfloat16)

    def lowered(rows, w_down):
        return jnp.dot(rows, w_down, preferred_element_type=jnp.float32).astype(jnp.bfloat16)

    new_state = next_state(decays, state_beside, rot_key, wide_values)
    shared_part = lowered(lifted(moe_beside, shared_gate, shared_up), shared_down)
    arrived, shared_part, new_state = lax.optimization_barrier((arrived, shared_part, new_state))

    own_in = arrived.reshape(experts_all, width)
    other_in = from_partner(own_in)
    own_hidden = lifted(own_in, expert_gate[0], expert_up[0])
    own_hidden, other_in = lax.optimization_barrier((own_hidden, other_in))
    other_hidden = lifted(other_in, expert_gate[0], expert_up[0])
    got = from_partner(lowered(other_hidden, expert_down[0]))
    own_sum = lowered(own_hidden, expert_down[0]).astype(jnp.float32) + got.astype(jnp.float32)
    own_sum = own_sum.astype(jnp.bfloat16)
    returned = exchanged(own_sum.reshape(experts_all, 2, -1), EP)
    back_rows = returned.reshape(experts_all, width).astype(jnp.float32)
    mixture_part = jnp.dot(combine, back_rows) + shared_part.astype(jnp.float32)
    mixture = mixture_part + from_partner(mixture_part)
    result = (middle + scaled_rows(mixture, out_gain)).astype(jnp.bfloat16)
    return (result, new_state)


def solution(mesh):
    finer = Mesh(mesh.devices.reshape(-1, 4, 4, mesh.shape["tp"]), ("ep_0", "ep_1", "ep_2", "tp"))
    in_specs = (
        P(EP, None),
        P(EP),
        P(EP, "tp", None, None),
        P(),
        P(),
        P(),
        P(),
        P(EP, "tp"),
        P(EP, "tp"),
        P(EP, "tp"),
        P(EP, "tp"),
        P("tp", EP),
        P(EP, None),
        P(EP, None),
        P(EP, None, "tp"),
        P(EP, None, "tp"),
        P(EP, "tp", None),
        P(None, "tp"),
        P(None, "tp"),
        P("tp", None),
    )
    out_specs = (P(EP, None), P(EP, "tp", None, None))

    return jax.shard_map(
        on_device, mesh=finer, in_specs=in_specs, out_specs=out_specs, check_vma=False
    )
```

```python
import jax
import jax.numpy as jnp
from jax import lax
from jax.experimental import pallas as pl
from jax.experimental.pallas import tpu as pltpu
from jax.sharding import Mesh
from jax.sharding import PartitionSpec as P

HEAD = 64
HEADS = 16
Z, Y, X = "ep_0", "ep_1", "ep_2"
EP = (Z, Y, X)


EPS = 1e-06
THETA = 10000.0


def exchanged(blocks, axes):
    return lax.all_to_all(blocks, axes, split_axis=0, concat_axis=0, tiled=True)


def copies(value, count):
    return jnp.broadcast_to(value, (count, *value.shape))


def from_partner(value):
    return lax.ppermute(value, "tp", [(0, 1), (1, 0)])


def rolled_lanes(rows, start):
    doubled = jnp.concatenate([rows, rows], axis=1)
    return lax.dynamic_slice_in_dim(doubled, start, rows.shape[1], 1)


def from_ahead(value, axis, step):
    size = lax.axis_size(axis)
    return lax.ppermute(value, axis, [((i + step) % size, i) for i in range(size)])


def in_place_order(blocks, axis, dim):
    size = blocks.shape[dim]
    doubled = jnp.concatenate([blocks, blocks], axis=dim)
    start = (size - lax.axis_index(axis)) % size
    return lax.dynamic_slice_in_dim(doubled, start, size, dim)


def plane_tokens(by_y):
    size_y, size_x = by_y.shape[0], lax.axis_size(X)
    mine = lax.axis_index(Y)
    column = [lax.dynamic_index_in_dim(by_y, mine, 0, keepdims=False)]
    for step in range(1, size_y):
        behind = (mine - step) % size_y
        block = lax.dynamic_index_in_dim(by_y, behind, 0, keepdims=False)
        column.append(from_ahead(block, Y, step))
    column = in_place_order(jnp.stack(column), Y, 0)
    others = [from_ahead(column, X, step) for step in range(1, size_x)]
    plane = jnp.stack([column, *others])
    return in_place_order(plane, X, 0).swapaxes(0, 1)


def rounded(values):
    return lax.optimization_barrier(values.astype(jnp.bfloat16)).astype(jnp.float32)


def scaled_rows(values, gain_row):
    widened = values.astype(jnp.float32)
    return widened * lax.rsqrt(jnp.mean(widened * widened, axis=-1, keepdims=True) + EPS) * gain_row


def rotate(vectors, lengths):
    half_dim = vectors.shape[-1] // 2
    frequency = THETA ** (-jnp.arange(half_dim, dtype=jnp.float32) / half_dim)
    angles = lengths.astype(jnp.float32)[:, None] * frequency[None, :]
    cosine = jnp.cos(angles)[:, None, :]
    sine_part = jnp.sin(angles)[:, None, :]
    leading = vectors[..., :half_dim]
    trailing = vectors[..., half_dim:]
    return jnp.concatenate(
        [leading * cosine - trailing * sine_part, trailing * cosine + leading * sine_part], axis=-1
    )


def decay_table(head_count):
    head_order = jnp.arange(head_count, dtype=jnp.float32)
    return 1.0 - jnp.exp2(-5.0 - 7.0 * head_order / (head_count - 1))


def retain(queries, keys_new, values, out_gate, prior_state, lengths, decays):
    seq_count = queries.shape[0]
    head_count = decays.shape[0]
    layout = (seq_count, head_count, HEAD)
    rot_query = rotate(queries.astype(jnp.float32).reshape(layout), lengths)
    rot_key = rotate(keys_new.astype(jnp.float32).reshape(layout), lengths) * HEAD ** (-0.5)
    wide_values = values.astype(jnp.float32).reshape(layout)
    from_state = jnp.einsum("shd,shde->she", rot_query, prior_state)
    self_term = jnp.sum(rot_query * rot_key, axis=-1, keepdims=True)
    read_out = decays[None, :, None] * from_state + self_term * wide_values
    normed = read_out * lax.rsqrt(jnp.mean(read_out * read_out, axis=-1, keepdims=True) + EPS)
    gated_rows = normed.reshape(seq_count, head_count * HEAD) * jax.nn.silu(
        out_gate.astype(jnp.float32)
    )
    return (gated_rows.astype(jnp.bfloat16), rot_key, wide_values)


def next_state(decays, prior_state, rot_key, wide_values):
    return (
        decays[None, :, None, None] * prior_state
        + rot_key[..., :, None] * wide_values[..., None, :]
    )


def expert_body(rows, gate_a, up_a, down_a, gate_b, up_b, down_b, out, total):
    step = pl.program_id(0)

    @pl.when(step == 0)
    def _():
        total[...] = jnp.zeros_like(total)

    for gate, up, down in ((gate_a, up_a, down_a), (gate_b, up_b, down_b)):
        gated = jnp.dot(rows[...], gate[...], preferred_element_type=jnp.float32)
        lifted = jnp.dot(rows[...], up[...], preferred_element_type=jnp.float32)
        hidden = (jax.nn.silu(gated) * lifted).astype(jnp.bfloat16)
        total[...] += jnp.dot(hidden, down[...], preferred_element_type=jnp.float32)

    @pl.when(step == pl.num_programs(0) - 1)
    def _():
        out[...] = total[...].astype(jnp.bfloat16)


def whole_expert(rows, here, there):
    count, width = rows.shape
    units, block = here[0].shape[1], 128
    across = pl.BlockSpec((width, block), lambda i: (0, i))
    down = pl.BlockSpec((block, width), lambda i: (i, 0))
    whole = pl.BlockSpec((count, width), lambda i: (0, 0))
    return pl.pallas_call(
        expert_body,
        grid=(units // block,),
        in_specs=[whole, across, across, down, across, across, down],
        out_specs=whole,
        out_shape=jax.ShapeDtypeStruct((count, width), jnp.bfloat16),
        scratch_shapes=[pltpu.VMEM((count, width), jnp.float32)],
        compiler_params=pltpu.CompilerParams(dimension_semantics=("arbitrary",)),
    )(rows, *here, *there)


def on_device(
    tokens,
    lengths,
    prior_state,
    mix_gain,
    post_gain,
    ffn_gain,
    out_gain,
    query_weight,
    key_weight,
    value_weight,
    gate_weight,
    out_weight,
    routes,
    route_gates,
    expert_gate,
    expert_up,
    expert_down,
    shared_gate,
    shared_up,
    shared_down,
):
    seq_here, width = tokens.shape
    cols = query_weight.shape[1]
    depth, rows_y, rows_x = (lax.axis_size(axis) for axis in EP)
    experts_all = depth * rows_y * rows_x
    plane = rows_y * rows_x
    core = lax.axis_index("tp")

    kinds = jnp.stack([query_weight, key_weight, value_weight, gate_weight])
    share = cols // rows_x
    wout_parts = out_weight.reshape(rows_x, share, -1).swapaxes(1, 2)
    sent = copies(jnp.concatenate([kinds, wout_parts], axis=2), depth)
    held = exchanged(sent.reshape(depth * rows_x, -1, cols + share), (Z, X))
    held = held.reshape(-1, cols + share)
    kind_weight = held[:, :cols]
    wout_part = held[:, cols:]
    others = [from_ahead(wout_part, X, step) for step in range(1, rows_x)]

    wide_tokens = tokens.astype(jnp.float32)
    gained = (wide_tokens * mix_gain).astype(jnp.bfloat16)
    by_y = gained.reshape(seq_here, depth, rows_y, -1).transpose(2, 0, 1, 3)
    plane_rows = plane_tokens(by_y.reshape(rows_y, seq_here, width // rows_y))
    projected = jnp.dot(
        plane_rows.reshape(plane * seq_here, -1), kind_weight, preferred_element_type=jnp.float32
    ).astype(jnp.bfloat16)
    projected, routes, route_gates, lengths = lax.optimization_barrier(
        (projected, routes, route_gates, lengths)
    )
    parts = exchanged(projected.reshape(plane, seq_here, cols), (Y, X))
    flat_routes = routes.reshape(-1)
    onehot = (flat_routes[:, None] == jnp.arange(experts_all, dtype=jnp.int32)[None, :]).astype(
        jnp.int32
    )
    earlier = jnp.cumsum(onehot, axis=0) - onehot
    ranks = jnp.sum(earlier * onehot, axis=1)
    mine = jnp.where(ranks == core, flat_routes, -1)
    placing = (jnp.arange(experts_all, dtype=jnp.int32)[:, None] == mine[None, :]).reshape(
        experts_all, seq_here, -1
    )
    dispatch_rows = jnp.any(placing, axis=2).astype(jnp.bfloat16)
    combine = jnp.sum(
        jnp.where(placing, route_gates[None, :, :], jnp.zeros((), jnp.float32)), axis=2
    ).T

    row_scale = lax.rsqrt(jnp.mean(wide_tokens * wide_tokens, axis=-1, keepdims=True) + EPS)

    parts, dispatch_rows, combine, row_scale = lax.optimization_barrier(
        (parts, dispatch_rows, combine, row_scale)
    )
    parts = parts.reshape(rows_y, rows_x, seq_here, cols).astype(jnp.float32)
    queries, keys_new, values, out_gate = (jnp.sum(parts, axis=0) * row_scale).astype(jnp.bfloat16)

    heads_here = cols // HEAD
    decays = lax.dynamic_slice_in_dim(decay_table(HEADS), core * heads_here, heads_here, 0)
    retained, rot_key, wide_values = retain(
        queries, keys_new, values, out_gate, prior_state, lengths, decays
    )

    turned = rolled_lanes(retained, lax.axis_index(X) * share)
    turned, others = lax.optimization_barrier((turned, others))
    wout_turned = jnp.concatenate([wout_part, *others], axis=1)
    retained_y = exchanged(copies(turned, rows_y), Y).reshape(rows_y * seq_here, cols)
    partial_mix = lax.dot_general(
        retained_y, wout_turned, (((1,), (1,)), ((), ())), preferred_element_type=jnp.float32
    ).astype(jnp.bfloat16)
    to_both = partial_mix.reshape(rows_y, 1, seq_here, -1)
    to_both = jnp.broadcast_to(to_both, (rows_y, 2, *to_both.shape[2:]))
    halves = exchanged(to_both.reshape(2 * rows_y, seq_here, -1), (Y, "tp"))
    halves = halves.reshape(rows_y, 2, seq_here, depth, -1).astype(jnp.float32)
    mixed = jnp.sum(halves, axis=1).astype(jnp.bfloat16)
    mixed = mixed.transpose(1, 2, 0, 3).reshape(seq_here, width)
    mixed_sum = rounded(mixed)
    middle = rounded(tokens.astype(jnp.float32) + scaled_rows(mixed_sum, post_gain))
    moe_in = scaled_rows(middle, ffn_gain).astype(jnp.bfloat16)

    outgoing = jnp.dot(dispatch_rows, moe_in, preferred_element_type=jnp.float32).astype(
        jnp.bfloat16
    )
    expert_here = (expert_gate[0], expert_up[0], expert_down[0])
    outgoing, moe_beside, prior_state, expert_here = lax.optimization_barrier(
        (outgoing, moe_in, prior_state, expert_here)
    )
    arrived = exchanged(outgoing.reshape(experts_all, 2, -1), EP)

    expert_there = tuple(from_partner(weight) for weight in expert_here)
    new_state = next_state(decays, prior_state, rot_key, wide_values)
    shared_gated = jnp.dot(moe_beside, shared_gate, preferred_element_type=jnp.float32)
    shared_lifted = jnp.dot(moe_beside, shared_up, preferred_element_type=jnp.float32)
    shared_hidden = (jax.nn.silu(shared_gated) * shared_lifted).astype(jnp.bfloat16)
    shared_part = jnp.dot(shared_hidden, shared_down, preferred_element_type=jnp.float32).astype(
        jnp.bfloat16
    )
    arrived, shared_part, new_state, expert_there = lax.optimization_barrier(
        (arrived, shared_part, new_state, expert_there)
    )

    own_sum = whole_expert(arrived.reshape(experts_all, width), expert_here, expert_there)
    returned = exchanged(own_sum.reshape(experts_all, 2, -1), EP)
    back_rows = returned.reshape(experts_all, width).astype(jnp.float32)
    mixture_part = jnp.dot(combine, back_rows) + shared_part.astype(jnp.float32)
    mixture = mixture_part + from_partner(mixture_part)
    result = (middle + scaled_rows(mixture, out_gain)).astype(jnp.bfloat16)
    return (result, new_state)


def solution(mesh):
    finer = Mesh(mesh.devices.reshape(-1, 4, 4, mesh.shape["tp"]), ("ep_0", "ep_1", "ep_2", "tp"))
    in_specs = (
        P(EP, None),
        P(EP),
        P(EP, "tp", None, None),
        P(),
        P(),
        P(),
        P(),
        P(EP, "tp"),
        P(EP, "tp"),
        P(EP, "tp"),
        P(EP, "tp"),
        P("tp", EP),
        P(EP, None),
        P(EP, None),
        P(EP, None, "tp"),
        P(EP, None, "tp"),
        P(EP, "tp", None),
        P(None, "tp"),
        P(None, "tp"),
        P("tp", None),
    )
    out_specs = (P(EP, None), P(EP, "tp", None, None))

    return jax.shard_map(
        on_device, mesh=finer, in_specs=in_specs, out_specs=out_specs, check_vma=False
    )
```

```python
import jax
import jax.numpy as jnp
from jax import lax
from jax.experimental import pallas as pl
from jax.experimental.pallas import tpu as pltpu
from jax.sharding import Mesh
from jax.sharding import PartitionSpec as P

HEAD = 64
HEADS = 16
Z, Y, X = "ep_0", "ep_1", "ep_2"
EP = (Z, Y, X)


EPS = 1e-06
THETA = 10000.0


def exchanged(blocks, axes):
    return lax.all_to_all(blocks, axes, split_axis=0, concat_axis=0, tiled=True)


def copies(value, count):
    return jnp.broadcast_to(value, (count, *value.shape))


def from_partner(value):
    return lax.ppermute(value, "tp", [(0, 1), (1, 0)])


def rolled_lanes(rows, start):
    doubled = jnp.concatenate([rows, rows], axis=1)
    return lax.dynamic_slice_in_dim(doubled, start, rows.shape[1], 1)


def from_ahead(value, axis, step):
    size = lax.axis_size(axis)
    return lax.ppermute(value, axis, [((i + step) % size, i) for i in range(size)])


def in_place_order(blocks, axis, dim):
    size = blocks.shape[dim]
    doubled = jnp.concatenate([blocks, blocks], axis=dim)
    start = (size - lax.axis_index(axis)) % size
    return lax.dynamic_slice_in_dim(doubled, start, size, dim)


def plane_tokens(by_y):
    size_y, size_x = by_y.shape[0], lax.axis_size(X)
    mine = lax.axis_index(Y)
    column = [lax.dynamic_index_in_dim(by_y, mine, 0, keepdims=False)]
    for step in range(1, size_y):
        behind = (mine - step) % size_y
        block = lax.dynamic_index_in_dim(by_y, behind, 0, keepdims=False)
        column.append(from_ahead(block, Y, step))
    column = in_place_order(jnp.stack(column), Y, 0)
    others = [from_ahead(column, X, step) for step in range(1, size_x)]
    plane = jnp.stack([column, *others])
    return in_place_order(plane, X, 0).swapaxes(0, 1)


def rounded(values):
    return lax.optimization_barrier(values.astype(jnp.bfloat16)).astype(jnp.float32)


def scaled_rows(values, gain_row):
    widened = values.astype(jnp.float32)
    return widened * lax.rsqrt(jnp.mean(widened * widened, axis=-1, keepdims=True) + EPS) * gain_row


def rotate(vectors, lengths):
    half_dim = vectors.shape[-1] // 2
    frequency = THETA ** (-jnp.arange(half_dim, dtype=jnp.float32) / half_dim)
    angles = lengths.astype(jnp.float32)[:, None] * frequency[None, :]
    cosine = jnp.cos(angles)[:, None, :]
    sine_part = jnp.sin(angles)[:, None, :]
    leading = vectors[..., :half_dim]
    trailing = vectors[..., half_dim:]
    return jnp.concatenate(
        [leading * cosine - trailing * sine_part, trailing * cosine + leading * sine_part], axis=-1
    )


def decay_table(head_count):
    head_order = jnp.arange(head_count, dtype=jnp.float32)
    return 1.0 - jnp.exp2(-5.0 - 7.0 * head_order / (head_count - 1))


def retain(queries, keys_new, values, out_gate, prior_state, lengths, decays):
    seq_count = queries.shape[0]
    head_count = decays.shape[0]
    layout = (seq_count, head_count, HEAD)
    rot_query = rotate(queries.astype(jnp.float32).reshape(layout), lengths)
    rot_key = rotate(keys_new.astype(jnp.float32).reshape(layout), lengths) * HEAD ** (-0.5)
    wide_values = values.astype(jnp.float32).reshape(layout)
    from_state = jnp.einsum("shd,shde->she", rot_query, prior_state)
    self_term = jnp.sum(rot_query * rot_key, axis=-1, keepdims=True)
    read_out = decays[None, :, None] * from_state + self_term * wide_values
    normed = read_out * lax.rsqrt(jnp.mean(read_out * read_out, axis=-1, keepdims=True) + EPS)
    gated_rows = normed.reshape(seq_count, head_count * HEAD) * jax.nn.silu(
        out_gate.astype(jnp.float32)
    )
    return (gated_rows.astype(jnp.bfloat16), rot_key, wide_values)


def next_state(decays, prior_state, rot_key, wide_values):
    return (
        decays[None, :, None, None] * prior_state
        + rot_key[..., :, None] * wide_values[..., None, :]
    )


def expert_body(rows, *refs):
    weights, out, held, arrivals = refs[:6], refs[6], refs[7:13], refs[13]
    copying = [
        pltpu.make_async_copy(weight, place, arrivals.at[k])
        for k, (weight, place) in enumerate(zip(weights, held))
    ]
    for copy in copying:
        copy.start()

    def hidden_of(gate_at, up_at):
        copying[gate_at].wait()
        gated = jnp.dot(rows[...], held[gate_at][...], preferred_element_type=jnp.float32)
        copying[up_at].wait()
        lifted = jnp.dot(rows[...], held[up_at][...], preferred_element_type=jnp.float32)
        return (jax.nn.silu(gated) * lifted).astype(jnp.bfloat16)

    hidden_here = hidden_of(0, 1)
    hidden_there = hidden_of(2, 3)
    copying[4].wait()
    total = jnp.dot(hidden_here, held[4][...], preferred_element_type=jnp.float32)
    copying[5].wait()
    total += jnp.dot(hidden_there, held[5][...], preferred_element_type=jnp.float32)
    out[...] = total.astype(jnp.bfloat16)


def whole_expert(rows, here, there):
    weights = (*here[:2], *there[:2], here[2], there[2])
    return pl.pallas_call(
        expert_body,
        in_specs=[pl.BlockSpec(memory_space=pltpu.VMEM)]
        + [pl.BlockSpec(memory_space=pl.ANY)] * len(weights),
        out_specs=pl.BlockSpec(memory_space=pltpu.VMEM),
        out_shape=jax.ShapeDtypeStruct(rows.shape, jnp.bfloat16),
        scratch_shapes=[pltpu.VMEM(weight.shape, weight.dtype) for weight in weights]
        + [pltpu.SemaphoreType.DMA((len(weights),))],
        compiler_params=pltpu.CompilerParams(vmem_limit_bytes=52 * 2**20),
    )(rows, *weights)


def on_device(
    tokens,
    lengths,
    prior_state,
    mix_gain,
    post_gain,
    ffn_gain,
    out_gain,
    query_weight,
    key_weight,
    value_weight,
    gate_weight,
    out_weight,
    routes,
    route_gates,
    expert_gate,
    expert_up,
    expert_down,
    shared_gate,
    shared_up,
    shared_down,
):
    seq_here, width = tokens.shape
    cols = query_weight.shape[1]
    depth, rows_y, rows_x = (lax.axis_size(axis) for axis in EP)
    experts_all = depth * rows_y * rows_x
    plane = rows_y * rows_x
    core = lax.axis_index("tp")

    kinds = jnp.stack([query_weight, key_weight, value_weight, gate_weight])
    share = cols // rows_x
    wout_parts = out_weight.reshape(rows_x, share, -1).swapaxes(1, 2)
    sent = copies(jnp.concatenate([kinds, wout_parts], axis=2), depth)
    held = exchanged(sent.reshape(depth * rows_x, -1, cols + share), (Z, X))
    held = held.reshape(-1, cols + share)
    kind_weight = held[:, :cols]
    wout_part = held[:, cols:]
    others = [from_ahead(wout_part, X, step) for step in range(1, rows_x)]

    wide_tokens = tokens.astype(jnp.float32)
    gained = (wide_tokens * mix_gain).astype(jnp.bfloat16)
    by_y = gained.reshape(seq_here, depth, rows_y, -1).transpose(2, 0, 1, 3)
    plane_rows = plane_tokens(by_y.reshape(rows_y, seq_here, width // rows_y))
    projected = jnp.dot(
        plane_rows.reshape(plane * seq_here, -1), kind_weight, preferred_element_type=jnp.float32
    ).astype(jnp.bfloat16)
    projected, routes, route_gates, lengths = lax.optimization_barrier(
        (projected, routes, route_gates, lengths)
    )
    parts = exchanged(projected.reshape(plane, seq_here, cols), (Y, X))
    flat_routes = routes.reshape(-1)
    onehot = (flat_routes[:, None] == jnp.arange(experts_all, dtype=jnp.int32)[None, :]).astype(
        jnp.int32
    )
    earlier = jnp.cumsum(onehot, axis=0) - onehot
    ranks = jnp.sum(earlier * onehot, axis=1)
    mine = jnp.where(ranks == core, flat_routes, -1)
    placing = (jnp.arange(experts_all, dtype=jnp.int32)[:, None] == mine[None, :]).reshape(
        experts_all, seq_here, -1
    )
    dispatch_rows = jnp.any(placing, axis=2).astype(jnp.bfloat16)
    combine = jnp.sum(
        jnp.where(placing, route_gates[None, :, :], jnp.zeros((), jnp.float32)), axis=2
    ).T

    row_scale = lax.rsqrt(jnp.mean(wide_tokens * wide_tokens, axis=-1, keepdims=True) + EPS)

    parts, dispatch_rows, combine, row_scale = lax.optimization_barrier(
        (parts, dispatch_rows, combine, row_scale)
    )
    parts = parts.reshape(rows_y, rows_x, seq_here, cols).astype(jnp.float32)
    queries, keys_new, values, out_gate = (jnp.sum(parts, axis=0) * row_scale).astype(jnp.bfloat16)

    heads_here = cols // HEAD
    decays = lax.dynamic_slice_in_dim(decay_table(HEADS), core * heads_here, heads_here, 0)
    retained, rot_key, wide_values = retain(
        queries, keys_new, values, out_gate, prior_state, lengths, decays
    )

    turned = rolled_lanes(retained, lax.axis_index(X) * share)
    turned, others = lax.optimization_barrier((turned, others))
    wout_turned = jnp.concatenate([wout_part, *others], axis=1)
    retained_y = exchanged(copies(turned, rows_y), Y).reshape(rows_y * seq_here, cols)
    partial_mix = lax.dot_general(
        retained_y, wout_turned, (((1,), (1,)), ((), ())), preferred_element_type=jnp.float32
    ).astype(jnp.bfloat16)
    to_both = partial_mix.reshape(rows_y, 1, seq_here, -1)
    to_both = jnp.broadcast_to(to_both, (rows_y, 2, *to_both.shape[2:]))
    halves = exchanged(to_both.reshape(2 * rows_y, seq_here, -1), (Y, "tp"))
    halves = halves.reshape(rows_y, 2, seq_here, depth, -1).astype(jnp.float32)
    mixed = jnp.sum(halves, axis=1).astype(jnp.bfloat16)
    mixed = mixed.transpose(1, 2, 0, 3).reshape(seq_here, width)
    mixed_sum = rounded(mixed)
    middle = rounded(tokens.astype(jnp.float32) + scaled_rows(mixed_sum, post_gain))
    moe_in = scaled_rows(middle, ffn_gain).astype(jnp.bfloat16)

    outgoing = jnp.dot(dispatch_rows, moe_in, preferred_element_type=jnp.float32).astype(
        jnp.bfloat16
    )
    expert_here = (expert_gate[0], expert_up[0], expert_down[0])
    outgoing, moe_beside, prior_state, expert_here = lax.optimization_barrier(
        (outgoing, moe_in, prior_state, expert_here)
    )
    arrived = exchanged(outgoing.reshape(experts_all, 2, -1), EP)

    expert_there = tuple(from_partner(weight) for weight in expert_here)
    new_state = next_state(decays, prior_state, rot_key, wide_values)
    shared_gated = jnp.dot(moe_beside, shared_gate, preferred_element_type=jnp.float32)
    shared_lifted = jnp.dot(moe_beside, shared_up, preferred_element_type=jnp.float32)
    shared_hidden = (jax.nn.silu(shared_gated) * shared_lifted).astype(jnp.bfloat16)
    shared_part = jnp.dot(shared_hidden, shared_down, preferred_element_type=jnp.float32).astype(
        jnp.bfloat16
    )
    arrived, shared_part, new_state, expert_there = lax.optimization_barrier(
        (arrived, shared_part, new_state, expert_there)
    )

    own_sum = whole_expert(arrived.reshape(experts_all, width), expert_here, expert_there)
    returned = exchanged(own_sum.reshape(experts_all, 2, -1), EP)
    back_rows = returned.reshape(experts_all, width).astype(jnp.float32)
    mixture_part = jnp.dot(combine, back_rows) + shared_part.astype(jnp.float32)
    mixture = mixture_part + from_partner(mixture_part)
    result = (middle + scaled_rows(mixture, out_gain)).astype(jnp.bfloat16)
    return (result, new_state)


def solution(mesh):
    finer = Mesh(mesh.devices.reshape(-1, 4, 4, mesh.shape["tp"]), ("ep_0", "ep_1", "ep_2", "tp"))
    in_specs = (
        P(EP, None),
        P(EP),
        P(EP, "tp", None, None),
        P(),
        P(),
        P(),
        P(),
        P(EP, "tp"),
        P(EP, "tp"),
        P(EP, "tp"),
        P(EP, "tp"),
        P("tp", EP),
        P(EP, None),
        P(EP, None),
        P(EP, None, "tp"),
        P(EP, None, "tp"),
        P(EP, "tp", None),
        P(None, "tp"),
        P(None, "tp"),
        P("tp", None),
    )
    out_specs = (P(EP, None), P(EP, "tp", None, None))

    return jax.shard_map(
        on_device, mesh=finer, in_specs=in_specs, out_specs=out_specs, check_vma=False
    )
```

```python
import jax
import jax.numpy as jnp
from jax import lax
from jax.experimental import pallas as pl
from jax.experimental.pallas import tpu as pltpu
from jax.sharding import Mesh
from jax.sharding import PartitionSpec as P

HEAD = 64
HEADS = 16
Z, Y, X = "ep_0", "ep_1", "ep_2"
EP = (Z, Y, X)


EPS = 1e-06
THETA = 10000.0


def exchanged(blocks, axes):
    return lax.all_to_all(blocks, axes, split_axis=0, concat_axis=0, tiled=True)


def copies(value, count):
    return jnp.broadcast_to(value, (count, *value.shape))


def from_partner(value):
    return lax.ppermute(value, "tp", [(0, 1), (1, 0)])


def rolled_lanes(rows, start):
    doubled = jnp.concatenate([rows, rows], axis=1)
    return lax.dynamic_slice_in_dim(doubled, start, rows.shape[1], 1)


def from_ahead(value, axis, step):
    size = lax.axis_size(axis)
    return lax.ppermute(value, axis, [((i + step) % size, i) for i in range(size)])


def in_place_order(blocks, axis, dim):
    size = blocks.shape[dim]
    doubled = jnp.concatenate([blocks, blocks], axis=dim)
    start = (size - lax.axis_index(axis)) % size
    return lax.dynamic_slice_in_dim(doubled, start, size, dim)


def plane_tokens(by_y):
    size_y, size_x = by_y.shape[0], lax.axis_size(X)
    mine = lax.axis_index(Y)
    column = [lax.dynamic_index_in_dim(by_y, mine, 0, keepdims=False)]
    for step in range(1, size_y):
        behind = (mine - step) % size_y
        block = lax.dynamic_index_in_dim(by_y, behind, 0, keepdims=False)
        column.append(from_ahead(block, Y, step))
    column = in_place_order(jnp.stack(column), Y, 0)
    others = [from_ahead(column, X, step) for step in range(1, size_x)]
    plane = jnp.stack([column, *others])
    return in_place_order(plane, X, 0).swapaxes(0, 1)


def rounded(values):
    return lax.optimization_barrier(values.astype(jnp.bfloat16)).astype(jnp.float32)


def scaled_rows(values, gain_row):
    widened = values.astype(jnp.float32)
    return widened * lax.rsqrt(jnp.mean(widened * widened, axis=-1, keepdims=True) + EPS) * gain_row


def rotate(vectors, lengths):
    half_dim = vectors.shape[-1] // 2
    frequency = THETA ** (-jnp.arange(half_dim, dtype=jnp.float32) / half_dim)
    angles = lengths.astype(jnp.float32)[:, None] * frequency[None, :]
    cosine = jnp.cos(angles)[:, None, :]
    sine_part = jnp.sin(angles)[:, None, :]
    leading = vectors[..., :half_dim]
    trailing = vectors[..., half_dim:]
    return jnp.concatenate(
        [leading * cosine - trailing * sine_part, trailing * cosine + leading * sine_part], axis=-1
    )


def decay_table(head_count):
    head_order = jnp.arange(head_count, dtype=jnp.float32)
    return 1.0 - jnp.exp2(-5.0 - 7.0 * head_order / (head_count - 1))


def retain(queries, keys_new, values, out_gate, prior_state, lengths, decays):
    seq_count = queries.shape[0]
    head_count = decays.shape[0]
    layout = (seq_count, head_count, HEAD)
    rot_query = rotate(queries.astype(jnp.float32).reshape(layout), lengths)
    rot_key = rotate(keys_new.astype(jnp.float32).reshape(layout), lengths) * HEAD ** (-0.5)
    wide_values = values.astype(jnp.float32).reshape(layout)
    from_state = jnp.einsum("shd,shde->she", rot_query, prior_state)
    self_term = jnp.sum(rot_query * rot_key, axis=-1, keepdims=True)
    read_out = decays[None, :, None] * from_state + self_term * wide_values
    normed = read_out * lax.rsqrt(jnp.mean(read_out * read_out, axis=-1, keepdims=True) + EPS)
    gated_rows = normed.reshape(seq_count, head_count * HEAD) * jax.nn.silu(
        out_gate.astype(jnp.float32)
    )
    return (gated_rows.astype(jnp.bfloat16), rot_key, wide_values)


def next_state(decays, prior_state, rot_key, wide_values):
    return (
        decays[None, :, None, None] * prior_state
        + rot_key[..., :, None] * wide_values[..., None, :]
    )


def expert_body(rows, *refs):
    weights, out, held, arrivals = refs[:6], refs[6], refs[7:13], refs[13]
    copying = [
        pltpu.make_async_copy(weight, place, arrivals.at[k])
        for k, (weight, place) in enumerate(zip(weights, held))
    ]
    for copy in copying:
        copy.start()

    def hidden_of(gate_at, up_at):
        copying[gate_at].wait()
        gated = jnp.dot(rows[...], held[gate_at][...], preferred_element_type=jnp.float32)
        copying[up_at].wait()
        lifted = jnp.dot(rows[...], held[up_at][...], preferred_element_type=jnp.float32)
        return (jax.nn.silu(gated) * lifted).astype(jnp.bfloat16)

    hidden_here = hidden_of(0, 1)
    hidden_there = hidden_of(2, 3)
    copying[4].wait()
    total = jnp.dot(hidden_here, held[4][...], preferred_element_type=jnp.float32)
    copying[5].wait()
    total += jnp.dot(hidden_there, held[5][...], preferred_element_type=jnp.float32)
    out[...] = total.astype(jnp.bfloat16)


def whole_expert(rows, here, there):
    weights = (*here[:2], *there[:2], here[2], there[2])
    return pl.pallas_call(
        expert_body,
        in_specs=[pl.BlockSpec(memory_space=pltpu.VMEM)]
        + [pl.BlockSpec(memory_space=pl.ANY)] * len(weights),
        out_specs=pl.BlockSpec(memory_space=pltpu.VMEM),
        out_shape=jax.ShapeDtypeStruct(rows.shape, jnp.bfloat16),
        scratch_shapes=[pltpu.VMEM(weight.shape, weight.dtype) for weight in weights]
        + [pltpu.SemaphoreType.DMA((len(weights),))],
        compiler_params=pltpu.CompilerParams(vmem_limit_bytes=52 * 2**20),
    )(rows, *weights)


def pack_body(query, key, value, gate, wout, tokens, gain, sent, gained):
    turned = wout[...].astype(jnp.float32).T.astype(jnp.bfloat16)
    cols = query.shape[1]
    share = sent.shape[2] - cols
    kinds = (query, key, value, gate)
    for place in range(sent.shape[0]):
        k = place % len(kinds)
        sent[place, :, :cols] = kinds[k][...]
        sent[place, :, cols:] = turned[:, k * share : (k + 1) * share]
    gained[...] = (tokens[...].astype(jnp.float32) * gain[...]).astype(jnp.bfloat16)


def packed(kinds, out_weight, tokens, gain, depth):
    rows, cols = kinds[0].shape
    count = len(kinds)
    return pl.pallas_call(
        pack_body,
        out_shape=(
            jax.ShapeDtypeStruct((depth * count, rows, cols + cols // count), jnp.bfloat16),
            jax.ShapeDtypeStruct(tokens.shape, jnp.bfloat16),
        ),
    )(*kinds, out_weight, tokens, gain[None, :])


def on_device(
    tokens,
    lengths,
    prior_state,
    mix_gain,
    post_gain,
    ffn_gain,
    out_gain,
    query_weight,
    key_weight,
    value_weight,
    gate_weight,
    out_weight,
    routes,
    route_gates,
    expert_gate,
    expert_up,
    expert_down,
    shared_gate,
    shared_up,
    shared_down,
):
    seq_here, width = tokens.shape
    cols = query_weight.shape[1]
    depth, rows_y, rows_x = (lax.axis_size(axis) for axis in EP)
    experts_all = depth * rows_y * rows_x
    plane = rows_y * rows_x
    core = lax.axis_index("tp")

    share = cols // rows_x
    kinds = (query_weight, key_weight, value_weight, gate_weight)
    sent, gained = packed(kinds, out_weight, tokens, mix_gain, depth)
    held = exchanged(sent, (Z, X))
    held = held.reshape(-1, cols + share)
    kind_weight = held[:, :cols]
    wout_part = held[:, cols:]
    others = [from_ahead(wout_part, X, step) for step in range(1, rows_x)]

    wide_tokens = tokens.astype(jnp.float32)
    by_y = gained.reshape(seq_here, depth, rows_y, -1).transpose(2, 0, 1, 3)
    plane_rows = plane_tokens(by_y.reshape(rows_y, seq_here, width // rows_y))
    projected = jnp.dot(
        plane_rows.reshape(plane * seq_here, -1), kind_weight, preferred_element_type=jnp.float32
    ).astype(jnp.bfloat16)
    projected, routes, route_gates, lengths = lax.optimization_barrier(
        (projected, routes, route_gates, lengths)
    )
    parts = exchanged(projected.reshape(plane, seq_here, cols), (Y, X))
    flat_routes = routes.reshape(-1)
    onehot = (flat_routes[:, None] == jnp.arange(experts_all, dtype=jnp.int32)[None, :]).astype(
        jnp.int32
    )
    earlier = jnp.cumsum(onehot, axis=0) - onehot
    ranks = jnp.sum(earlier * onehot, axis=1)
    mine = jnp.where(ranks == core, flat_routes, -1)
    placing = (jnp.arange(experts_all, dtype=jnp.int32)[:, None] == mine[None, :]).reshape(
        experts_all, seq_here, -1
    )
    dispatch_rows = jnp.any(placing, axis=2).astype(jnp.bfloat16)
    combine = jnp.sum(
        jnp.where(placing, route_gates[None, :, :], jnp.zeros((), jnp.float32)), axis=2
    ).T

    row_scale = lax.rsqrt(jnp.mean(wide_tokens * wide_tokens, axis=-1, keepdims=True) + EPS)

    parts, dispatch_rows, combine, row_scale = lax.optimization_barrier(
        (parts, dispatch_rows, combine, row_scale)
    )
    parts = parts.reshape(rows_y, rows_x, seq_here, cols).astype(jnp.float32)
    queries, keys_new, values, out_gate = (jnp.sum(parts, axis=0) * row_scale).astype(jnp.bfloat16)

    heads_here = cols // HEAD
    decays = lax.dynamic_slice_in_dim(decay_table(HEADS), core * heads_here, heads_here, 0)
    retained, rot_key, wide_values = retain(
        queries, keys_new, values, out_gate, prior_state, lengths, decays
    )

    turned = rolled_lanes(retained, lax.axis_index(X) * share)
    turned, others = lax.optimization_barrier((turned, others))
    wout_turned = jnp.concatenate([wout_part, *others], axis=1)
    retained_y = exchanged(copies(turned, rows_y), Y).reshape(rows_y * seq_here, cols)
    partial_mix = lax.dot_general(
        retained_y, wout_turned, (((1,), (1,)), ((), ())), preferred_element_type=jnp.float32
    ).astype(jnp.bfloat16)
    to_both = partial_mix.reshape(rows_y, 1, seq_here, -1)
    to_both = jnp.broadcast_to(to_both, (rows_y, 2, *to_both.shape[2:]))
    halves = exchanged(to_both.reshape(2 * rows_y, seq_here, -1), (Y, "tp"))
    halves = halves.reshape(rows_y, 2, seq_here, depth, -1).astype(jnp.float32)
    mixed = jnp.sum(halves, axis=1).astype(jnp.bfloat16)
    mixed = mixed.transpose(1, 2, 0, 3).reshape(seq_here, width)
    mixed_sum = rounded(mixed)
    middle = rounded(tokens.astype(jnp.float32) + scaled_rows(mixed_sum, post_gain))
    moe_in = scaled_rows(middle, ffn_gain).astype(jnp.bfloat16)

    outgoing = jnp.dot(dispatch_rows, moe_in, preferred_element_type=jnp.float32).astype(
        jnp.bfloat16
    )
    expert_here = (expert_gate[0], expert_up[0], expert_down[0])
    outgoing, moe_beside, prior_state, expert_here = lax.optimization_barrier(
        (outgoing, moe_in, prior_state, expert_here)
    )
    arrived = exchanged(outgoing.reshape(experts_all, 2, -1), EP)

    expert_there = tuple(from_partner(weight) for weight in expert_here)
    new_state = next_state(decays, prior_state, rot_key, wide_values)
    shared_gated = jnp.dot(moe_beside, shared_gate, preferred_element_type=jnp.float32)
    shared_lifted = jnp.dot(moe_beside, shared_up, preferred_element_type=jnp.float32)
    shared_hidden = (jax.nn.silu(shared_gated) * shared_lifted).astype(jnp.bfloat16)
    shared_part = jnp.dot(shared_hidden, shared_down, preferred_element_type=jnp.float32).astype(
        jnp.bfloat16
    )
    arrived, shared_part, new_state, expert_there = lax.optimization_barrier(
        (arrived, shared_part, new_state, expert_there)
    )

    own_sum = whole_expert(arrived.reshape(experts_all, width), expert_here, expert_there)
    returned = exchanged(own_sum.reshape(experts_all, 2, -1), EP)
    back_rows = returned.reshape(experts_all, width).astype(jnp.float32)
    mixture_part = jnp.dot(combine, back_rows) + shared_part.astype(jnp.float32)
    mixture = mixture_part + from_partner(mixture_part)
    result = (middle + scaled_rows(mixture, out_gain)).astype(jnp.bfloat16)
    return (result, new_state)


def solution(mesh):
    finer = Mesh(mesh.devices.reshape(-1, 4, 4, mesh.shape["tp"]), ("ep_0", "ep_1", "ep_2", "tp"))
    in_specs = (
        P(EP, None),
        P(EP),
        P(EP, "tp", None, None),
        P(),
        P(),
        P(),
        P(),
        P(EP, "tp"),
        P(EP, "tp"),
        P(EP, "tp"),
        P(EP, "tp"),
        P("tp", EP),
        P(EP, None),
        P(EP, None),
        P(EP, None, "tp"),
        P(EP, None, "tp"),
        P(EP, "tp", None),
        P(None, "tp"),
        P(None, "tp"),
        P("tp", None),
    )
    out_specs = (P(EP, None), P(EP, "tp", None, None))

    return jax.shard_map(
        on_device, mesh=finer, in_specs=in_specs, out_specs=out_specs, check_vma=False
    )
```
